32 devices in a mesh: gr: 2 (over x), fs: 8 (over z, y), tp: 2 (over core).
Axes of the slice: x: 2, y: 2, z: 4, core: 2. Of those that a mesh axis runs over, the one named last changes fastest.
Arguments:
- prompt: bfloat16 [3072, 2048], P(('gr', 'fs', 'tp')), may hold values from -6 to 6
- norm_first: float32 [2048], P(('gr', 'fs')), may hold values from 0.1 to 1.9
- gate_first: float32 [2048, 5632], P(('gr', 'fs'), 'tp'), may hold values from -6 to 6
- up_first: float32 [2048, 5632], P(('gr', 'fs'), 'tp'), may hold values from -6 to 6
- down_first: float32 [2048, 5632], P(('gr', 'fs'), 'tp'), may hold values from -6 to 6
- norm_second: float32 [2048], P(('gr', 'fs')), may hold values from 0.1 to 1.9
- gate_second: float32 [2048, 5632], P(('gr', 'fs'), 'tp'), may hold values from -6 to 6
- up_second: float32 [2048, 5632], P(('gr', 'fs'), 'tp'), may hold values from -6 to 6
- down_second: float32 [2048, 5632], P(('gr', 'fs'), 'tp'), may hold values from -6 to 6
Outputs:
- served_gate_first: bfloat16 [2048, 5632], P(None, 'fs')
- served_up_first: bfloat16 [2048, 5632], P(None, 'fs')
- served_down_first: bfloat16 [2048, 5632], P(None, 'fs')
- served_gate_second: bfloat16 [2048, 5632], P(None, 'fs')
- served_up_second: bfloat16 [2048, 5632], P(None, 'fs')
- served_down_second: bfloat16 [2048, 5632], P(None, 'fs')
- result: bfloat16 [3072, 2048], P(('gr', 'fs', 'tp'))
The draws below stay inside these ranges and needn't reach their ends.
All inputs are finite; a program needn't handle non-finite values.
Results may differ from the reference program's by a relative error of at most 0.015.
Values may be sent and summed in bfloat16 or wider, within the bound.
A program may use at most 128 MiB of HBM per device.

```python
import jax
import jax.numpy as jnp
from jax import lax

D = 2048
FF = 5632
FF_BLK = 704
TOKENS = 3072


def block_scale(key, shape, cuts, least, high):
    factor_of = 1.0
    for axis_at, parts in cuts:
        heights = jax.random.uniform(jax.random.fold_in(jax.random.fold_in(key, 6), axis_at), (parts,), jnp.float32, least / len(cuts), high / len(cuts))
        factor_of = factor_of * jnp.repeat(jnp.exp(heights), shape[axis_at] // parts).reshape((-1,) + (1,) * (len(shape) - 1 - axis_at))
    return factor_of


def scatter_about(stream_key, extent, spread, most, pieces=(), kind=jnp.bfloat16):
    level = block_scale(stream_key, extent, pieces, -0.22, 0.18) if pieces else 1.0
    drawn = jax.random.normal(stream_key, extent, jnp.float32) * spread * level
    return jnp.minimum(jnp.maximum(drawn, -most), most).astype(kind)


def setup_inputs(seed: int = 0) -> dict:
    seeds = jax.random.split(jax.random.key(seed), 10)
    prompt = scatter_about(seeds[0], (TOKENS, D), 1.0, 6.0, ((0, 32),))
    norm_first = jnp.clip(1.0 + 0.18 * jax.random.normal(seeds[1], (D,), jnp.float32), 0.1, 1.9)
    gate_first = scatter_about(seeds[2], (D, FF), 1.0, 6.0, ((0, 16), (1, 2)), jnp.float32)
    up_first = scatter_about(seeds[3], (D, FF), 1.0, 6.0, ((0, 16), (1, 2)), jnp.float32)
    down_first = scatter_about(seeds[4], (D, FF), 1.0, 6.0, ((0, 16), (1, 2)), jnp.float32)
    norm_second = jnp.clip(1.0 + 0.18 * jax.random.normal(seeds[5], (D,), jnp.float32), 0.1, 1.9)
    gate_second = scatter_about(seeds[6], (D, FF), 1.0, 6.0, ((0, 16), (1, 2)), jnp.float32)
    up_second = scatter_about(seeds[7], (D, FF), 1.0, 6.0, ((0, 16), (1, 2)), jnp.float32)
    down_second = scatter_about(seeds[8], (D, FF), 1.0, 6.0, ((0, 16), (1, 2)), jnp.float32)
    return dict(prompt=prompt, norm_first=norm_first, gate_first=gate_first, up_first=up_first, down_first=down_first, norm_second=norm_second, gate_second=gate_second, up_second=up_second, down_second=down_second)


EPS = 1e-06

def fold_rows(gain, weight):
    return (gain[:, None] * weight).astype(jnp.bfloat16)

def half_step(residual, gate_weight, up_weight, down_weight):
    resid_f = residual.astype(jnp.float32)
    normed = (resid_f * lax.rsqrt(lax.optimization_barrier(jnp.mean(resid_f * resid_f, axis=-1, keepdims=True)) + EPS)).astype(jnp.bfloat16)
    gate_pre = jnp.dot(normed, gate_weight, preferred_element_type=jnp.float32) * D ** (-0.5)
    up_pre = jnp.dot(normed, up_weight, preferred_element_type=jnp.float32) * D ** (-0.5)
    hidden = (jax.nn.silu(gate_pre) * up_pre).astype(jnp.bfloat16)

    def add_block(running, block_index):
        offset = block_index * FF_BLK
        hid_block = lax.dynamic_slice_in_dim(hidden, offset, FF_BLK, 1)
        down_block = lax.dynamic_slice_in_dim(down_weight, offset, FF_BLK, 1)
        partial_sum = lax.dot_general(hid_block, down_block, (((1,), (1,)), ((), ())), preferred_element_type=jnp.float32) * FF ** (-0.5)
        partial_sum = lax.optimization_barrier(partial_sum.astype(jnp.bfloat16)).astype(jnp.float32)
        return (running + partial_sum, None)
    start_sum = jnp.zeros((residual.shape[0], D), jnp.float32)
    branch, _ = lax.scan(add_block, start_sum, jnp.arange(FF // FF_BLK, dtype=jnp.int32))
    return (resid_f + 0.5 * branch).astype(jnp.bfloat16)

def reference(prompt, norm_first, gate_first, up_first, down_first, norm_second, gate_second, up_second, down_second):
    served_gate_first = fold_rows(norm_first, gate_first)
    served_up_first = fold_rows(norm_first, up_first)
    served_down_first = down_first.astype(jnp.bfloat16)
    served_gate_second = fold_rows(norm_second, gate_second)
    served_up_second = fold_rows(norm_second, up_second)
    served_down_second = down_second.astype(jnp.bfloat16)
    middle = half_step(prompt, served_gate_first, served_up_first, served_down_first)
    result = half_step(middle, served_gate_second, served_up_second, served_down_second)
    return (served_gate_first, served_up_first, served_down_first, served_gate_second, served_up_second, served_down_second, result)
```

```python
import functools

import jax
import jax.numpy as jnp
from jax import lax
from jax.experimental import pallas as pl
from jax.experimental.pallas import tpu as pltpu
from jax.sharding import PartitionSpec as P

EPS = 1e-06
MESH = pl.DeviceIdType.MESH
VMEM_LIMIT = 63 * 1024 * 1024
ANY = pl.BlockSpec(memory_space=pl.ANY)
VMEM = pl.BlockSpec(memory_space=pltpu.VMEM)


def inner_of(fs):
    return max(n for n in range(1, fs + 1) if fs % n == 0 and n * n <= fs)


class Place:
    def __init__(self, sizes):
        self.gr, self.fs, self.tp = sizes
        self.ny = inner_of(self.fs)
        self.nz = self.fs // self.ny
        self.g, self.f, self.t = (lax.axis_index(axis) for axis in ("gr", "fs", "tp"))
        self.z = self.f // self.ny
        self.y = self.f % self.ny

    def at(self, z, y):
        return (self.g, z * self.ny + y, self.t)


def remote(src, dst, send_sem, recv_sem, device):
    return pltpu.make_async_remote_copy(
        src_ref=src,
        dst_ref=dst,
        send_sem=send_sem,
        recv_sem=recv_sem,
        device_id=device,
        device_id_type=MESH,
    )


def wait_bytes(ref, sem):
    pltpu.make_async_copy(ref, ref, sem).wait()


def rows_of_block(ref, f, count):
    return ref.at[pl.ds(pl.multiple_of(f * count, count), count)]


class Relayout:
    def __init__(self, place, pieces, out, sems):
        self.p, self.pieces, self.out = place, pieces, out
        self.first_send, self.first_recv, self.gr_send, self.gr_recv, self.tp_send, self.tp_recv = sems
        self.blocks, self.rows, self.width = pieces.shape
        self.sub = self.rows // place.tp

    def rows_of(self, from_gr, from_fs, core):
        start = pl.multiple_of((from_gr * self.p.fs + from_fs) * self.rows + core * self.sub, self.sub)
        return self.out.at[pl.ds(start, self.sub)]

    def _first(self, step, act_local, act_far):
        p = self.p
        slot = (step + p.f) % self.blocks
        block = p.t * self.blocks + slot
        for core in range(p.tp):
            mine = jnp.logical_and(block == p.f, p.t == core)
            source = self.pieces.at[slot, pl.ds(core * self.sub, self.sub)]
            target = self.rows_of(p.g, p.f, core)
            far = remote(
                source,
                target,
                self.first_send.at[slot, core],
                self.first_recv.at[p.f],
                (p.g, block, core),
            )
            if act_local is not None:

                @pl.when(mine)
                def _():
                    act_local(source, target)

            @pl.when(jnp.logical_not(mine))
            def _():
                act_far(far)

    def send(self):
        def local(source, target):
            pltpu.make_async_copy(source, target, self.first_recv.at[self.p.f]).start()

        def body(step, carry):
            self._first(step, local, lambda copy: copy.start())
            return carry

        lax.fori_loop(0, self.blocks, body, 0)

    def origin(self, step):
        p, blocks = self.p, self.blocks
        return ((p.f // blocks + step % p.tp) % p.tp) * blocks + (p.f + blocks - step // p.tp) % blocks

    def _to_peers(self, ref):
        p = self.p
        for hop in range(1, p.tp):
            remote(ref, ref, self.tp_send, self.tp_recv, (p.g, p.f, (p.t + hop) % p.tp)).start()

    def pass_on(self):
        p = self.p

        def body(step, carry):
            source = self.origin(step)
            ref = self.rows_of(p.g, source, p.t)
            wait_bytes(ref, self.first_recv.at[source])
            for hop in range(1, p.gr):
                remote(
                    ref,
                    ref,
                    self.gr_send,
                    self.gr_recv.at[hop - 1, source],
                    ((p.g + hop) % p.gr, p.f, p.t),
                ).start()
            self._to_peers(ref)
            return carry

        lax.fori_loop(0, p.fs, body, 0)

    def pass_far(self):
        p = self.p

        def body(step, carry):
            source = self.origin(step)
            for hop in range(1, p.gr):
                ref = self.rows_of((p.g + p.gr - hop) % p.gr, source, p.t)
                wait_bytes(ref, self.gr_recv.at[hop - 1, source])
                self._to_peers(ref)
            return carry

        lax.fori_loop(0, p.fs, body, 0)

    def _wait_rows(self, count, sem):
        if count:
            wait_bytes(self.out.at[pl.ds(0, count)], sem)

    def wait_all_here(self):
        p = self.p
        self._wait_rows(p.gr * p.fs * self.sub * (p.tp - 1), self.tp_recv)

    def drain(self):
        p = self.p

        def body(step, carry):
            self._first(step, None, lambda copy: copy.wait_send())
            return carry

        lax.fori_loop(0, self.blocks, body, 0)
        self._wait_rows(p.fs * self.sub * (p.gr - 1), self.gr_send)
        self._wait_rows(p.gr * p.fs * self.sub * (p.tp - 1), self.tp_send)


def relayout_sems(mats, blocks, sizes):
    gr, fs, tp = sizes
    return [
        pltpu.SemaphoreType.DMA((mats, blocks, tp)),
        pltpu.SemaphoreType.DMA((mats, fs)),
        pltpu.SemaphoreType.DMA((mats,)),
        pltpu.SemaphoreType.DMA((mats, max(gr - 1, 1), fs)),
        pltpu.SemaphoreType.DMA((mats,)),
        pltpu.SemaphoreType.DMA((mats,)),
    ]


class Gather:
    def __init__(self, place, tokens, count, send_sem, recv_sem):
        self.p, self.tokens, self.count = place, tokens, count
        self.send_sem, self.recv_sem = send_sem, recv_sem

    def block(self, f):
        return rows_of_block(self.tokens, f, self.count)

    def _copy(self, f, way, z, y):
        ref = self.block(f)
        return remote(ref, ref, self.send_sem.at[f, way], self.recv_sem.at[f], self.p.at(z, y))

    def _forwards(self, z0, y0, dz, dy, act):
        p = self.p
        f = z0 * p.ny + y0
        for sign in dz:
            z = p.z + sign

            @pl.when((z >= 0) & (z < p.nz))
            def _():
                act(self._copy(f, 0 if sign > 0 else 1, z, p.y))

        for sign in dy:
            y = p.y + sign

            @pl.when((y >= 0) & (y < p.ny))
            def _():
                act(self._copy(f, 2 if sign > 0 else 3, p.z, y))

    def _each(self, stage, visit):
        p = self.p
        if stage == 0:
            visit(None, p.z, p.y, (1, -1), (1, -1))
        elif stage < p.nz:
            for sign in (1, -1):
                z0 = p.z - sign * stage
                visit((z0 >= 0) & (z0 < p.nz), z0, p.y, (sign,), (1, -1))
        else:
            hops = stage - p.nz + 1
            for away in range(p.nz):
                for sign_z in (1, -1) if away else (1,):
                    z0 = p.z - sign_z * away
                    for sign in (1, -1):
                        y0 = p.y - sign * hops
                        ways = (sign,) if hops + 1 < p.ny else ()
                        visit((z0 >= 0) & (z0 < p.nz) & (y0 >= 0) & (y0 < p.ny), z0, y0, (), ways)

    def stages(self):
        return self.p.nz + self.p.ny - 1

    def run(self, stage, arrived=None):
        def visit(valid, z0, y0, dz, dy):
            def go():
                f = z0 * self.p.ny + y0
                if stage:
                    wait_bytes(self.block(f), self.recv_sem.at[f])
                self._forwards(z0, y0, dz, dy, lambda copy: copy.start())
                if arrived is not None:
                    arrived(f)

            if valid is None:
                go()
            else:
                pl.when(valid)(go)

        self._each(stage, visit)

    def drain(self):
        def visit(valid, z0, y0, dz, dy):
            def go():
                self._forwards(z0, y0, dz, dy, lambda copy: copy.wait_send())

            if valid is None:
                go()
            else:
                pl.when(valid)(go)

        for stage in range(self.stages()):
            self._each(stage, visit)


class Scatter:
    def __init__(self, place, part, y_land, z_land, count, sems):
        self.p, self.part, self.y_land, self.z_land, self.count = place, part, y_land, z_land, count
        self.y_send, self.y_recv, self.z_send, self.z_recv = sems

    def block(self, f):
        return rows_of_block(self.part, f, self.count)

    def _y_copy(self, z0, y0, sign):
        p = self.p
        f = z0 * p.ny + y0
        at = p.y + sign
        slot = f if sign < 0 else jnp.where(at == y0, p.fs + z0, f)
        return remote(
            self.block(f), self.y_land.at[slot], self.y_send.at[f], self.y_recv.at[slot], p.at(p.z, at)
        )

    def _z_copy(self, z0, sign):
        p = self.p
        at = p.z + sign
        slot = z0 if sign < 0 else jnp.where(at == z0, p.nz, z0)
        return remote(
            self.block(z0 * p.ny + p.y),
            self.z_land.at[slot],
            self.z_send.at[z0],
            self.z_recv.at[slot],
            p.at(at, p.y),
        )

    def _add(self, f, land, recv, slot):
        wait_bytes(land.at[slot], recv.at[slot])
        rows = pl.ds(pl.multiple_of(f * self.count, self.count), self.count)
        total = self.part[rows].astype(jnp.float32) + land[slot].astype(jnp.float32)
        self.part[rows] = total.astype(jnp.bfloat16)

    def send_y(self, z0):
        p = self.p
        for hops in range(p.ny - 1, 0, -1):
            for sign in (1, -1):
                y0, behind = p.y + sign * hops, p.y - sign
                valid = (y0 >= 0) & (y0 < p.ny)
                f = z0 * p.ny + y0
                if hops + 1 < p.ny:

                    @pl.when(valid & (behind >= 0) & (behind < p.ny))
                    def _():
                        self._add(f, self.y_land, self.y_recv, f)

                @pl.when(valid)
                def _():
                    self._y_copy(z0, y0, sign).start()

    def take_y(self, z0):
        p = self.p
        f = z0 * p.ny + p.y

        @pl.when(p.y + 1 < p.ny)
        def _():
            self._add(f, self.y_land, self.y_recv, f)

        @pl.when(p.y > 0)
        def _():
            self._add(f, self.y_land, self.y_recv, p.fs + z0)

    def by_distance(self, visit):
        p = self.p
        for hops in range(p.nz - 1, 0, -1):
            for sign in (1, -1):
                z0 = p.z + sign * hops
                pl.when((z0 >= 0) & (z0 < p.nz))(functools.partial(visit, z0, sign, hops))

    def reduce(self):
        p = self.p

        def step(z0, sign, hops):
            self.take_y(z0)
            behind = p.z - sign
            if hops + 1 < p.nz:

                @pl.when((behind >= 0) & (behind < p.nz))
                def _():
                    self._add(z0 * p.ny + p.y, self.z_land, self.z_recv, z0)

            self._z_copy(z0, sign).start()

        self.by_distance(step)
        self.take_y(p.z)

        @pl.when(p.z + 1 < p.nz)
        def _():
            self._add(p.f, self.z_land, self.z_recv, p.z)

        @pl.when(p.z > 0)
        def _():
            self._add(p.f, self.z_land, self.z_recv, p.nz)

    def drain(self):
        p = self.p
        for z0 in range(p.nz):
            for hops in range(1, p.ny):
                for sign in (1, -1):
                    y0 = p.y + sign * hops

                    @pl.when((y0 >= 0) & (y0 < p.ny))
                    def _():
                        self._y_copy(z0, y0, sign).wait_send()

        self.by_distance(lambda z0, sign, hops: self._z_copy(z0, sign).wait_send())


def scatter_scratch(sizes, count, depth):
    fs = sizes[1]
    ny = inner_of(fs)
    nz = fs // ny
    return [
        pltpu.VMEM((fs + nz, count, depth), jnp.bfloat16),
        pltpu.VMEM((nz + 1, count, depth), jnp.bfloat16),
        pltpu.SemaphoreType.DMA((fs,)),
        pltpu.SemaphoreType.DMA((fs + nz,)),
        pltpu.SemaphoreType.DMA((nz,)),
        pltpu.SemaphoreType.DMA((nz + 1,)),
    ]


def normed_tokens(resid_f):
    return (
        resid_f * lax.rsqrt(jnp.mean(resid_f * resid_f, axis=-1, keepdims=True) + EPS)
    ).astype(jnp.bfloat16)


def column_of(row):
    n = row.shape[1]
    across = lax.broadcasted_iota(jnp.int32, (n, n), 1)
    down = lax.broadcasted_iota(jnp.int32, (n, n), 0)
    return jnp.sum(jnp.where(across == down, row, 0.0), axis=1, keepdims=True)


def cut_into(pieces, weight, gain):
    blocks, _, width = pieces.shape
    for slot in range(blocks):
        value = weight[:, slot * width : (slot + 1) * width]
        if gain is not None:
            value = gain * value
        pieces[slot] = value.astype(jnp.bfloat16)


def ffn_rows(tokens, weights, part, hidden, start, scales):
    gate, up, down = weights
    in_scale, out_scale = scales
    count, width = hidden.shape
    depth = tokens.shape[1]
    rows = pl.ds(start, count)
    for low in range(0, width, 256):
        high = min(low + 256, width)
        gate_pre = jnp.dot(tokens[rows, :], gate[:, low:high], preferred_element_type=jnp.float32) * in_scale
        up_pre = jnp.dot(tokens[rows, :], up[:, low:high], preferred_element_type=jnp.float32) * in_scale
        act = gate_pre / (1.0 + jnp.exp(-gate_pre)) * up_pre
        hidden[:, low:high] = act.astype(jnp.bfloat16)
    chunk = 256 if depth % 256 == 0 else depth

    def body(i, carry):
        low = pl.multiple_of(i * chunk, chunk)
        value = lax.dot_general(
            hidden[...],
            down[pl.ds(low, chunk), :],
            (((1,), (1,)), ((), ())),
            preferred_element_type=jnp.float32,
        )
        part[rows, pl.ds(low, chunk)] = (value * out_scale).astype(jnp.bfloat16)
        return carry

    lax.fori_loop(0, depth // chunk, body, 0)


def scales_of(depth, width, fs):
    return depth ** (-0.5), (width * fs) ** (-0.5)


def first_kernel(sizes, count, rows_at_once, *refs):
    (prompt, gain_first, gain_second, *weights), refs = refs[:9], refs[9:]
    (*served, tokens_out, middle_out), refs = refs[:8], refs[8:]
    (prompt_v, weights_v, pieces, first_v, tokens, tokens_next, part, hidden), refs = refs[:8], refs[8:]
    (in_sem, out_sem, token_sem, ag_send, ag_recv, *refs) = refs
    relayout_refs, scatter_refs = refs[:6], refs[6:]
    p = Place(sizes)
    total, width = served[0].shape
    depth = tokens.shape[1]
    scales = scales_of(depth, width, p.fs)

    loads = [pltpu.make_async_copy(prompt, prompt_v, in_sem.at[6])]
    loads += [pltpu.make_async_copy(weights[m], weights_v.at[m], in_sem.at[m]) for m in range(6)]
    for load in loads:
        load.start()

    targets = [first_v.at[m] for m in range(3)] + list(served[3:])
    moves = [
        Relayout(p, pieces.at[m], targets[m], [s.at[m] for s in relayout_refs]) for m in range(6)
    ]
    gains = [gain_first, gain_first, None, gain_second, gain_second, None]

    def cut(m):
        loads[1 + m].wait()
        gain = None if gains[m] is None else column_of(gains[m][...])
        cut_into(pieces.at[m], weights_v.at[m], gain)

    own = pl.ds(pl.multiple_of(p.f * count, count), count)
    gather = Gather(p, tokens, count, ag_send.at[0], ag_recv.at[0])
    loads[0].wait()
    tokens[own] = normed_tokens(prompt_v[...].astype(jnp.float32))
    gather.run(0)
    cut(0)
    moves[0].send()
    cut(1)
    gather.run(1)
    moves[1].send()
    cut(2)
    moves[0].pass_on()
    for stage in range(2, p.nz - 1):
        gather.run(stage)
    moves[2].send()
    moves[1].pass_on()
    for stage in range(max(p.nz - 1, 2), p.nz):
        gather.run(stage)
    cut(3)
    cut(4)
    cut(5)
    moves[2].pass_on()
    for stage in range(p.nz, gather.stages()):
        gather.run(stage)
    for m in range(3):
        moves[m].pass_far()
    for m in range(3):
        moves[m].wait_all_here()
    outs = [pltpu.make_async_copy(first_v.at[m], served[m], out_sem.at[m]) for m in range(3)]
    for out in outs:
        out.start()
    moves[3].send()

    scatter = Scatter(p, part, scatter_refs[0], scatter_refs[1], count, scatter_refs[2:])
    blocks_at_once = rows_at_once // count
    tiles = p.fs // blocks_at_once
    z_at_once = blocks_at_once // p.ny

    def tile(step, carry):
        at = (tiles - 1 - step) if tiles == 1 else jnp.where(2 * p.z < p.nz, tiles - 1 - step, step)
        start = pl.multiple_of(at * rows_at_once, rows_at_once)
        ffn_rows(tokens, [first_v.at[m] for m in range(3)], part, hidden, start, scales)
        for i in range(z_at_once):
            scatter.send_y(at * z_at_once + jnp.where(2 * p.z < p.nz, z_at_once - 1 - i, i))
        return carry

    lax.fori_loop(0, tiles, tile, 0)
    moves[4].send()
    scatter.reduce()
    middle = (prompt_v[...].astype(jnp.float32) + 0.5 * part[own].astype(jnp.float32)).astype(jnp.bfloat16)
    middle_out[...] = middle
    tokens_next[own] = normed_tokens(middle.astype(jnp.float32))
    gather_next = Gather(p, tokens_next, count, ag_send.at[1], ag_recv.at[1])

    def store(f):
        pltpu.make_async_copy(
            rows_of_block(tokens_next, f, count), rows_of_block(tokens_out, f, count), token_sem
        ).start()

    gather_next.run(0, store)
    moves[3].pass_on()
    for stage in range(1, p.nz):
        if stage == 1:
            moves[5].send()
        gather_next.run(stage, store)
        if stage == 2:
            moves[4].pass_on()
    moves[5].pass_on()
    for stage in range(p.nz, gather_next.stages()):
        gather_next.run(stage, store)
    for m in range(3, 6):
        moves[m].pass_far()
    for m in range(3, 6):
        moves[m].wait_all_here()
    wait_bytes(tokens_next, token_sem)
    for out in outs:
        out.wait()
    for move in moves:
        move.drain()
    gather.drain()
    gather_next.drain()
    scatter.drain()


def first_half(prompt, gains, weights, sizes):
    gr, fs, tp = sizes
    rows, columns = weights[0].shape
    count, depth = prompt.shape
    blocks = fs // tp
    width = columns // blocks
    total = gr * fs * rows
    rows_at_once = count * fs // 2
    bf16 = jnp.bfloat16
    served = jax.ShapeDtypeStruct((total, width), bf16)
    return pl.pallas_call(
        functools.partial(first_kernel, sizes, count, rows_at_once),
        out_shape=[served] * 6
        + [jax.ShapeDtypeStruct((count * fs, depth), bf16), jax.ShapeDtypeStruct((count, depth), bf16)],
        in_specs=[ANY, VMEM, VMEM] + [ANY] * 6,
        out_specs=[ANY] * 7 + [VMEM],
        scratch_shapes=[
            pltpu.VMEM((count, depth), bf16),
            pltpu.VMEM((6, rows, columns), jnp.float32),
            pltpu.VMEM((6, blocks, rows, width), bf16),
            pltpu.VMEM((3, total, width), bf16),
            pltpu.VMEM((count * fs, depth), bf16),
            pltpu.VMEM((count * fs, depth), bf16),
            pltpu.VMEM((count * fs, depth), bf16),
            pltpu.VMEM((rows_at_once, width), bf16),
            pltpu.SemaphoreType.DMA((7,)),
            pltpu.SemaphoreType.DMA((3,)),
            pltpu.SemaphoreType.DMA,
            pltpu.SemaphoreType.DMA((2, fs, 4)),
            pltpu.SemaphoreType.DMA((2, fs)),
            *relayout_sems(6, blocks, sizes),
            *scatter_scratch(sizes, count, depth),
        ],
        compiler_params=pltpu.CompilerParams(has_side_effects=True, vmem_limit_bytes=VMEM_LIMIT),
        name="first_half",
    )(prompt, *(gain.reshape(1, -1) for gain in gains), *weights)


def second_kernel(fs, rows_at_once, *refs):
    (tokens, *served), refs = refs[:7], refs[7:]
    (*outs, part), refs = refs[:7], refs[7:]
    tokens_v, served_v, part_v, hidden, in_sem, out_sem, part_sem = refs
    order = [3, 4, 5, 0, 1, 2]
    depth, width = tokens.shape[1], served[0].shape[1]
    scales = scales_of(depth, width, fs)
    loads = {m: pltpu.make_async_copy(served[m], served_v.at[m], in_sem.at[m]) for m in order}
    stores = {m: pltpu.make_async_copy(served_v.at[m], outs[m], out_sem.at[m]) for m in order}
    load_tokens = pltpu.make_async_copy(tokens, tokens_v, in_sem.at[6])
    load_tokens.start()
    for m in order:
        loads[m].start()
    load_tokens.wait()
    for m in order[:3]:
        loads[m].wait()
        stores[m].start()
    tiles = tokens.shape[0] // rows_at_once

    def tile(step, carry):
        start = pl.multiple_of(step * rows_at_once, rows_at_once)
        ffn_rows(tokens_v, [served_v.at[m] for m in (3, 4, 5)], part_v, hidden, start, scales)
        rows = pl.ds(start, rows_at_once)
        pltpu.make_async_copy(part_v.at[rows], part.at[rows], part_sem).start()
        return carry

    lax.fori_loop(0, tiles, tile, 0)
    for m in order[3:]:
        loads[m].wait()
        stores[m].start()
    for m in order:
        stores[m].wait()
    wait_bytes(part_v, part_sem)


def second_half(tokens, served, fs):
    total, width = served[0].shape
    count, depth = tokens.shape
    rows_at_once = count // 2
    bf16 = jnp.bfloat16
    return pl.pallas_call(
        functools.partial(second_kernel, fs, rows_at_once),
        out_shape=[jax.ShapeDtypeStruct((total, width), bf16)] * 6
        + [jax.ShapeDtypeStruct((count, depth), bf16)],
        in_specs=[ANY] * 7,
        out_specs=[ANY] * 7,
        scratch_shapes=[
            pltpu.VMEM((count, depth), bf16),
            pltpu.VMEM((6, total, width), bf16),
            pltpu.VMEM((count, depth), bf16),
            pltpu.VMEM((rows_at_once, width), bf16),
            pltpu.SemaphoreType.DMA((7,)),
            pltpu.SemaphoreType.DMA((6,)),
            pltpu.SemaphoreType.DMA,
        ],
        compiler_params=pltpu.CompilerParams(vmem_limit_bytes=VMEM_LIMIT),
        name="second_half",
    )(tokens, *served)


def last_kernel(sizes, count, partial, middle, result, part, part_sem, *scatter_refs):
    p = Place(sizes)
    scatter = Scatter(p, part, scatter_refs[0], scatter_refs[1], count, scatter_refs[2:])

    def load(z0):
        rows = pl.ds(pl.multiple_of(z0 * p.ny * count, p.ny * count), p.ny * count)
        return pltpu.make_async_copy(partial.at[rows], part.at[rows], part_sem.at[z0])

    order = []
    for i in range(p.nz):
        order.append(jnp.where(2 * p.z < p.nz, p.nz - 1 - i, i))
    for z0 in order:
        load(z0).start()
    for z0 in order:
        load(z0).wait()
        scatter.send_y(z0)
    scatter.reduce()
    own = pl.ds(pl.multiple_of(p.f * count, count), count)
    result[...] = (
        middle[...].astype(jnp.float32) + 0.5 * part[own].astype(jnp.float32)
    ).astype(jnp.bfloat16)
    scatter.drain()


def last_step(partial, middle, sizes):
    fs = sizes[1]
    count, depth = middle.shape
    return pl.pallas_call(
        functools.partial(last_kernel, sizes, count),
        out_shape=jax.ShapeDtypeStruct((count, depth), jnp.bfloat16),
        in_specs=[ANY, VMEM],
        out_specs=VMEM,
        scratch_shapes=[
            pltpu.VMEM((fs * count, depth), jnp.bfloat16),
            pltpu.SemaphoreType.DMA((fs // inner_of(fs),)),
            *scatter_scratch(sizes, count, depth),
        ],
        compiler_params=pltpu.CompilerParams(has_side_effects=True, vmem_limit_bytes=VMEM_LIMIT),
        name="last_step",
    )(partial, middle)


def on_device(
    prompt,
    norm_first,
    gate_first,
    up_first,
    down_first,
    norm_second,
    gate_second,
    up_second,
    down_second,
):
    sizes = tuple(lax.axis_size(axis) for axis in ("gr", "fs", "tp"))
    weights = (gate_first, up_first, down_first, gate_second, up_second, down_second)
    *served, tokens, middle = first_half(prompt, (norm_first, norm_second), weights, sizes)
    *served, partial = second_half(tokens, served, sizes[1])
    result = last_step(partial, middle, sizes)
    return (*served, result)


def solution(mesh):
    in_specs = (
        P(("gr", "fs", "tp"), None),
        P(("gr", "fs")),
        P(("gr", "fs"), "tp"),
        P(("gr", "fs"), "tp"),
        P(("gr", "fs"), "tp"),
        P(("gr", "fs")),
        P(("gr", "fs"), "tp"),
        P(("gr", "fs"), "tp"),
        P(("gr", "fs"), "tp"),
    )
    out_specs = (
        P(None, "fs"),
        P(None, "fs"),
        P(None, "fs"),
        P(None, "fs"),
        P(None, "fs"),
        P(None, "fs"),
        P(("gr", "fs", "tp"), None),
    )
    return jax.shard_map(
        on_device, mesh=mesh, in_specs=in_specs, out_specs=out_specs, check_vma=False
    )
```

```python
import functools

import jax
import jax.numpy as jnp
from jax import lax
from jax.experimental import pallas as pl
from jax.experimental.pallas import tpu as pltpu
from jax.sharding import PartitionSpec as P

EPS = 1e-06
MESH = pl.DeviceIdType.MESH
VMEM_LIMIT = 63 * 1024 * 1024
CUTS = 2
SAME, NEAR, ACROSS = range(3)
ANY = pl.BlockSpec(memory_space=pl.ANY)
VMEM = pl.BlockSpec(memory_space=pltpu.VMEM)


def inner_of(fs):
    return max(n for n in range(1, fs + 1) if fs % n == 0 and n * n <= fs)


class Place:
    def __init__(self, sizes):
        self.gr, self.fs, self.tp = sizes
        self.ny = inner_of(self.fs)
        self.nz = self.fs // self.ny
        self.g, self.f, self.t = (lax.axis_index(axis) for axis in ("gr", "fs", "tp"))
        self.z = self.f // self.ny
        self.y = self.f % self.ny

    def at(self, z, y):
        return (self.g, z * self.ny + y, self.t)

    def partner(self, z):
        return z + 1 - 2 * (z % 2)

    def by_z(self, z, z0, cut):
        paired = z0 == self.partner(z)
        return paired if cut == 0 else paired & (z > 0) & (z < self.nz - 1)


def remote(src, dst, send_sem, recv_sem, device):
    return pltpu.make_async_remote_copy(
        src_ref=src,
        dst_ref=dst,
        send_sem=send_sem,
        recv_sem=recv_sem,
        device_id=device,
        device_id_type=MESH,
    )


def wait_bytes(ref, sem):
    pltpu.make_async_copy(ref, ref, sem).wait()


def rows_of_block(ref, f, count):
    return ref.at[pl.ds(pl.multiple_of(f * count, count), count)]


def greet(devices):
    barrier = pltpu.get_barrier_semaphore()
    expected = 0
    for valid, device in devices:

        def signal():
            pl.semaphore_signal(barrier, inc=1, device_id=device, device_id_type=MESH)

        if valid is True:
            signal()
            expected = expected + 1
        else:
            pl.when(valid)(signal)
            expected = expected + jnp.where(valid, 1, 0)
    return lambda: pl.semaphore_wait(barrier, expected)


def plane_and_replicas(p):
    for away in range(p.fs):
        for hop in range(p.tp):
            if away or hop:
                yield True, (p.g, (p.f + away) % p.fs, (p.t + hop) % p.tp)
    for hop in range(1, p.gr):
        yield True, ((p.g + hop) % p.gr, p.f, p.t)


def neighbours(p):
    for sign in (1, -1):
        yield (p.z + sign >= 0) & (p.z + sign < p.nz), p.at(p.z + sign, p.y)
        yield (p.y + sign >= 0) & (p.y + sign < p.ny), p.at(p.z, p.y + sign)


class Relayout:
    def __init__(self, place, turned, pieces, out, sems):
        self.p, self.turned, self.pieces, self.out = place, turned, pieces, out
        self.first_send, self.first_recv, self.gr_send, self.gr_recv, self.tp_send, self.tp_recv = sems
        self.blocks, height, across = pieces.shape
        self.sub = height // place.tp
        self.rows = across if turned else height

    def rows_of(self, from_gr, from_fs, core):
        source = from_gr * self.p.fs + from_fs
        if self.turned:
            start = pl.multiple_of(source * self.rows, self.rows)
            return self.out.at[pl.ds(core * self.sub, self.sub), pl.ds(start, self.rows)]
        start = pl.multiple_of(source * self.rows + core * self.sub, self.sub)
        return self.out.at[pl.ds(start, self.sub)]

    def _first(self, step, act_local, act_far, group):
        p = self.p
        slot = (step + p.f) % self.blocks
        block = p.t * self.blocks + slot
        z0 = block // p.ny
        across = (2 * z0 < p.nz) != (2 * p.z < p.nz)
        if group == SAME:
            wanted = z0 == p.z
        elif group == ACROSS:
            wanted = across
        elif group == NEAR:
            wanted = jnp.logical_not(across) & (z0 != p.z)
        for core in range(p.tp):
            mine = jnp.logical_and(block == p.f, p.t == core)
            source = self.pieces.at[slot, pl.ds(core * self.sub, self.sub)]
            target = self.rows_of(p.g, p.f, core)
            far = remote(
                source,
                target,
                self.first_send.at[slot, core],
                self.first_recv.at[p.f],
                (p.g, block, core),
            )
            if act_local is not None and group == SAME:

                @pl.when(mine)
                def _():
                    act_local(source, target)

            others = jnp.logical_not(mine)

            @pl.when(others if group is None else others & wanted)
            def _():
                act_far(far)

    @jax.named_scope("w_send")
    def send(self, group):
        def local(source, target):
            pltpu.make_async_copy(source, target, self.first_recv.at[self.p.f]).start()

        def body(step, carry):
            self._first(step, local, lambda copy: copy.start(), group)
            return carry

        lax.fori_loop(0, self.blocks, body, 0)

    def _to_peers(self, ref):
        p = self.p
        for hop in range(1, p.tp):
            remote(ref, ref, self.tp_send, self.tp_recv, (p.g, p.f, (p.t + hop) % p.tp)).start()

    def _near(self, hops, visit):
        p = self.p
        for sign in (1, -1) if hops else (1,):
            z0 = p.z + sign * hops

            @pl.when((z0 >= 0) & (z0 < p.nz))
            def _():
                def body(i, carry):
                    visit(z0 * p.ny + (p.y + i) % p.ny)
                    return carry

                lax.fori_loop(0, p.ny, body, 0)

    def pass_on(self, hops):
        p = self.p

        def visit(source):
            ref = self.rows_of(p.g, source, p.t)
            wait_bytes(ref, self.first_recv.at[source])
            for hop in range(1, p.gr):
                remote(
                    ref,
                    ref,
                    self.gr_send,
                    self.gr_recv.at[hop - 1, source],
                    ((p.g + hop) % p.gr, p.f, p.t),
                ).start()
            self._to_peers(ref)

        with jax.named_scope(f"w_pass_on#d={hops}"):
            self._near(hops, visit)

    def pass_far(self, hops):
        p = self.p

        def visit(source):
            for hop in range(1, p.gr):
                ref = self.rows_of((p.g + p.gr - hop) % p.gr, source, p.t)
                wait_bytes(ref, self.gr_recv.at[hop - 1, source])
                self._to_peers(ref)

        with jax.named_scope(f"w_pass_far#d={hops}"):
            self._near(hops, visit)

    def _wait_pieces(self, count, sem):
        if not count:
            return
        if self.turned:
            half = pl.ds(0, self.sub)
            per_row = self.p.gr * self.p.fs
            if count % per_row:
                wait_bytes(self.out.at[half, pl.ds(0, count * self.rows)], sem)
            else:
                wait_bytes(self.out.at[pl.ds(0, self.sub * (count // per_row))], sem)
        else:
            wait_bytes(self.out.at[pl.ds(0, count * self.sub)], sem)

    @jax.named_scope("w_wait")
    def wait_all_here(self):
        p = self.p
        self._wait_pieces(p.gr * p.fs * (p.tp - 1), self.tp_recv)

    def drain(self):
        p = self.p

        def body(step, carry):
            self._first(step, None, lambda copy: copy.wait_send(), None)
            return carry

        lax.fori_loop(0, self.blocks, body, 0)
        self._wait_pieces(p.fs * (p.gr - 1), self.gr_send)
        self._wait_pieces(p.gr * p.fs * (p.tp - 1), self.tp_send)


def relayout_sems(mats, blocks, sizes):
    gr, fs, tp = sizes
    return [
        pltpu.SemaphoreType.DMA((mats, blocks, tp)),
        pltpu.SemaphoreType.DMA((mats, fs)),
        pltpu.SemaphoreType.DMA((mats,)),
        pltpu.SemaphoreType.DMA((mats, max(gr - 1, 1), fs)),
        pltpu.SemaphoreType.DMA((mats,)),
        pltpu.SemaphoreType.DMA((mats,)),
    ]


class Gather:
    def __init__(self, place, tokens, cuts, send_sem, recv_sem):
        self.p, self.tokens, self.cuts = place, tokens, cuts
        self.height = tokens.shape[0] // (place.fs * cuts)
        self.send_sem, self.recv_sem = send_sem, recv_sem

    def piece(self, f, cut):
        return rows_of_block(self.tokens, f * self.cuts + cut, self.height)

    def _along_z(self, f, cut, sign, act, also=None):
        p = self.p
        z = p.z + sign
        ref = self.piece(f, cut)
        valid = (z >= 0) & (z < p.nz)

        @pl.when(valid if also is None else valid & also)
        def _():
            way = jnp.where(sign > 0, 0, 1)
            act(remote(ref, ref, self.send_sem.at[f, cut, way], self.recv_sem.at[f, cut], p.at(z, p.y)))

    def _along_y(self, f, cut, sign, act, also=None):
        p = self.p
        y = p.y + sign
        ref = self.piece(f, cut)
        valid = (y >= 0) & (y < p.ny)

        @pl.when(valid if also is None else valid & also)
        def _():
            way = 2 if sign > 0 else 3
            act(remote(ref, ref, self.send_sem.at[f, cut, way], self.recv_sem.at[f, cut], p.at(p.z, y)))

    def _each(self, stage, arrive, act, done):
        p = self.p
        last = p.nz

        def column(z0, sign, cut):
            f = z0 * p.ny + p.y
            arrive(f, cut)
            self._along_z(f, cut, sign, act)
            by_y = jnp.logical_not(p.by_z(p.z, z0, cut))
            for way in (1, -1):
                self._along_y(f, cut, way, act, by_y)
            done(f, cut)

        def row(z0, y0, sign, hops, same, cut):
            f = z0 * p.ny + y0
            arrive(f, cut)
            if hops + 1 < p.ny:
                self._along_y(f, cut, sign, act, jnp.logical_not(p.by_z(p.z, z0, cut)))
            if same:
                other = p.partner(p.z)
                self._along_z(f, cut, other - p.z, act, p.by_z(other, p.z, cut))
            done(f, cut)

        def rows(away):
            for hops in range(1, p.ny):
                for sign_z in (1, -1) if away else (1,):
                    z0 = p.z - sign_z * away
                    for sign in (1, -1):
                        y0 = p.y - sign * hops

                        @pl.when((z0 >= 0) & (z0 < p.nz) & (y0 >= 0) & (y0 < p.ny))
                        def _():
                            for cut in range(self.cuts):
                                row(z0, y0, sign, hops, away == 0, cut)

        if stage == 0:
            for cut in range(self.cuts):
                for sign in (1, -1):
                    self._along_z(p.f, cut, sign, act)
                    self._along_y(p.f, cut, sign, act)
                done(p.f, cut)
        elif stage < last:
            for sign in (1, -1):
                z0 = p.z - sign * stage

                @pl.when((z0 >= 0) & (z0 < p.nz))
                def _():
                    for cut in range(self.cuts):
                        column(z0, sign, cut)

            if stage == 1:
                rows(0)
        else:
            for away in range(1, p.nz):
                rows(away)

    def run(self, stage, done=lambda f, cut: None):
        with jax.named_scope(f"gather#s={stage}"):
            self._each(
                stage,
                lambda f, cut: wait_bytes(self.piece(f, cut), self.recv_sem.at[f, cut]),
                lambda copy: copy.start(),
                done,
            )

    def drain(self):
        for stage in range(self.p.nz + 1):
            self._each(stage, lambda f, cut: None, lambda copy: copy.wait_send(), lambda f, cut: None)


class Scatter:
    def __init__(self, place, part, y_land, z_land, row_land, sems):
        self.p, self.part, self.y_land, self.z_land, self.row_land = place, part, y_land, z_land, row_land
        self.y_send, self.y_recv, self.z_send, self.z_recv, self.row_recv = sems
        self.cuts, self.height = y_land.shape[1:3]
        self.towards = jnp.where(2 * place.z < place.nz, 1, -1)

    def rows(self, f, cut):
        return pl.ds(pl.multiple_of((f * self.cuts + cut) * self.height, self.height), self.height)

    def _y_copy(self, z0, y0, sign, cut):
        p = self.p
        f = z0 * p.ny + y0
        at = p.y + sign
        slot = f if sign < 0 else jnp.where(at == y0, p.fs + z0, f)
        return remote(
            self.part.at[self.rows(f, cut)],
            self.y_land.at[slot, cut],
            self.y_send.at[f, cut],
            self.y_recv.at[slot, cut],
            p.at(p.z, at),
        )

    def _z_copy(self, z0, sign, cut):
        p = self.p
        at = p.z + sign
        slot = jnp.where((sign > 0) & (at == z0), p.nz, z0)
        return remote(
            self.part.at[self.rows(z0 * p.ny + p.y, cut)],
            self.z_land.at[slot, cut],
            self.z_send.at[z0, cut],
            self.z_recv.at[slot, cut],
            p.at(at, p.y),
        )

    def _add(self, f, land, recv, slot, cut):
        wait_bytes(land.at[slot, cut], recv.at[slot, cut])
        rows = self.rows(f, cut)
        total = self.part[rows].astype(jnp.float32) + land[slot, cut].astype(jnp.float32)
        self.part[rows] = total.astype(jnp.bfloat16)

    def _row_copy(self, z0, y0, cut):
        p = self.p
        f = z0 * p.ny + y0
        return remote(
            self.part.at[self.rows(f, cut)],
            self.row_land.at[y0, cut],
            self.y_send.at[f, cut],
            self.row_recv.at[y0, cut],
            p.at(z0, p.y),
        )

    def send_y(self, z0):
        self._send_y(z0, False)

    def send_own_y(self):
        with jax.named_scope("own_row"):
            self._send_y(self.p.z, True)

    def _send_y(self, z0, own):
        p = self.p
        other = p.partner(p.z)
        for hops in range(p.ny - 1, 0, -1):
            for sign in (1, -1):
                y0, behind = p.y + sign * hops, p.y - sign
                valid = (y0 >= 0) & (y0 < p.ny)
                f = z0 * p.ny + y0
                for cut in range(self.cuts):
                    if own:

                        @pl.when(valid & (other < p.nz) & p.by_z(other, p.z, cut))
                        def _():
                            self._add(f, self.row_land, self.row_recv, y0, cut)

                    by_z = False if own else p.by_z(p.z, z0, cut)
                    by_y = valid if own else valid & jnp.logical_not(by_z)
                    if hops + 1 < p.ny:

                        @pl.when(by_y & (behind >= 0) & (behind < p.ny))
                        def _():
                            self._add(f, self.y_land, self.y_recv, f, cut)

                    @pl.when(by_y)
                    def _():
                        self._y_copy(z0, y0, sign, cut).start()

                    if not own:

                        @pl.when(valid & by_z)
                        def _():
                            self._row_copy(z0, y0, cut).start()

    def take_y(self, z0, cut):
        p = self.p
        f = z0 * p.ny + p.y
        by_y = jnp.logical_not(p.by_z(p.z, z0, cut))

        @pl.when(by_y & (p.y + 1 < p.ny))
        def _():
            self._add(f, self.y_land, self.y_recv, f, cut)

        @pl.when(by_y & (p.y > 0))
        def _():
            self._add(f, self.y_land, self.y_recv, p.fs + z0, cut)

    def at_distance(self, hops, visit, also=None):
        p = self.p
        for sign in (self.towards, -self.towards) if hops else (1,):
            z0 = p.z + sign * hops
            valid = (z0 >= 0) & (z0 < p.nz)
            if also is not None:
                valid = valid & also(z0)
            pl.when(valid)(functools.partial(visit, z0, sign))

    def send_y_of(self, also):
        for hops in range(self.p.nz - 1, 0, -1):
            self.at_distance(hops, lambda z0, sign: self.send_y(z0), also)

    def reduce(self, hops):
        p = self.p

        def step(z0, sign):
            behind = p.z - sign
            for cut in range(self.cuts):
                self.take_y(z0, cut)
                if hops + 1 < p.nz:

                    @pl.when((behind >= 0) & (behind < p.nz))
                    def _():
                        self._add(z0 * p.ny + p.y, self.z_land, self.z_recv, z0, cut)

                self._z_copy(z0, sign, cut).start()

        with jax.named_scope(f"reduce#d={hops}"):
            if hops:
                self.at_distance(hops, step)
                return
            for cut in range(self.cuts):
                self.take_y(p.z, cut)

                @pl.when(p.z + 1 < p.nz)
                def _():
                    self._add(p.f, self.z_land, self.z_recv, p.z, cut)

                @pl.when(p.z > 0)
                def _():
                    self._add(p.f, self.z_land, self.z_recv, p.nz, cut)

    def drain(self):
        p = self.p
        for cut in range(self.cuts):
            for z0 in range(p.nz):
                for hops in range(1, p.ny):
                    for sign in (1, -1):
                        y0 = p.y + sign * hops

                        @pl.when((y0 >= 0) & (y0 < p.ny))
                        def _():
                            self._y_copy(z0, y0, sign, cut).wait_send()

            for hops in range(1, p.nz):
                self.at_distance(hops, lambda z0, sign: self._z_copy(z0, sign, cut).wait_send())


def cuts_of(count):
    return CUTS if count % (16 * CUTS) == 0 else 1


def scatter_scratch(sizes, count, depth):
    fs = sizes[1]
    ny = inner_of(fs)
    nz = fs // ny
    cuts = cuts_of(count)
    piece = (cuts, count // cuts, depth)
    return [
        pltpu.VMEM((fs + nz, *piece), jnp.bfloat16),
        pltpu.VMEM((nz + 1, *piece), jnp.bfloat16),
        pltpu.VMEM((ny, *piece), jnp.bfloat16),
        pltpu.SemaphoreType.DMA((fs, cuts)),
        pltpu.SemaphoreType.DMA((fs + nz, cuts)),
        pltpu.SemaphoreType.DMA((nz, cuts)),
        pltpu.SemaphoreType.DMA((nz + 1, cuts)),
        pltpu.SemaphoreType.DMA((ny, cuts)),
    ]


def normed_tokens(resid_f):
    return (
        resid_f * lax.rsqrt(jnp.mean(resid_f * resid_f, axis=-1, keepdims=True) + EPS)
    ).astype(jnp.bfloat16)


def column_of(row):
    n = row.shape[1]
    across = lax.broadcasted_iota(jnp.int32, (n, n), 1)
    down = lax.broadcasted_iota(jnp.int32, (n, n), 0)
    return jnp.sum(jnp.where(across == down, row, 0.0), axis=1, keepdims=True)


@jax.named_scope("cut")
def cut_into(pieces, weight, gain, turned):
    blocks, height, width = pieces.shape
    if turned:
        value = weight[...].T
        if gain is not None:
            value = value * gain[...]
        for slot in range(blocks):
            pieces[slot] = value[slot * height : (slot + 1) * height].astype(jnp.bfloat16)
        return
    gain = None if gain is None else column_of(gain[...])
    for slot in range(blocks):
        value = weight[:, slot * width : (slot + 1) * width]
        if gain is not None:
            value = gain * value
        pieces[slot] = value.astype(jnp.bfloat16)


def slabs_of(width):
    return [(low, min(low + 256, width)) for low in range(0, width, 256)]


@jax.named_scope("ffn")
def ffn_rows(tokens, weights, part, hidden, start, scales, turned, ready=lambda i: None):
    gate, up, down = weights
    in_scale, out_scale = scales
    count, width = hidden.shape
    depth = tokens.shape[1]
    rows = pl.ds(start, count)
    inward = (((1,), (1 if turned else 0,)), ((), ()))
    outward = (((1,), (0 if turned else 1,)), ((), ()))
    for i, (low, high) in enumerate(slabs_of(width)):
        ready(i)

        def project(weight):
            block = weight[low:high, :] if turned else weight[:, low:high]
            return lax.dot_general(
                tokens[rows, :], block, inward, preferred_element_type=jnp.float32
            ) * in_scale

        gate_pre, up_pre = project(gate), project(up)
        act = gate_pre / (1.0 + jnp.exp(-gate_pre)) * up_pre
        hidden[:, low:high] = act.astype(jnp.bfloat16)
    ready(None)
    chunk = 256 if depth % 256 == 0 else depth

    def body(i, carry):
        low = pl.multiple_of(i * chunk, chunk)
        block = down[:, pl.ds(low, chunk)] if turned else down[pl.ds(low, chunk), :]
        value = lax.dot_general(hidden[...], block, outward, preferred_element_type=jnp.float32)
        part[rows, pl.ds(low, chunk)] = (value * out_scale).astype(jnp.bfloat16)
        return carry

    lax.fori_loop(0, depth // chunk, body, 0)


def scales_of(depth, width, fs):
    return depth ** (-0.5), (width * fs) ** (-0.5)


def turns(rows):
    return rows % 128 == 0


def first_kernel(sizes, count, rows_at_once, turned, *refs):
    (prompt, gain_first, gain_second, *weights), refs = refs[:9], refs[9:]
    (*served, tokens_out, middle_out), refs = refs[:8], refs[8:]
    (prompt_v, weights_v, pieces, first_v, tokens, tokens_next, part, hidden), refs = refs[:8], refs[8:]
    (in_sem, out_sem, token_sem, ag_send, ag_recv, *refs) = refs
    relayout_refs, scatter_refs = refs[:6], refs[6:]
    p = Place(sizes)
    depth = tokens.shape[1]
    scales = scales_of(depth, hidden.shape[1], p.fs)

    loads = [pltpu.make_async_copy(prompt, prompt_v, in_sem.at[6])]
    loads += [pltpu.make_async_copy(weights[m], weights_v.at[m], in_sem.at[m]) for m in range(6)]
    with jax.named_scope("start"):
        for load in loads:
            load.start()

    targets = [first_v.at[m] for m in range(3)] + list(served[3:])
    moves = [
        Relayout(p, turned, pieces.at[m], targets[m], [s.at[m] for s in relayout_refs])
        for m in range(6)
    ]
    gains = [gain_first, gain_first, None, gain_second, gain_second, None]

    def cut(m):
        loads[1 + m].wait()
        cut_into(pieces.at[m], weights_v.at[m], gains[m], turned)

    own = pl.ds(pl.multiple_of(p.f * count, count), count)
    cuts = cuts_of(count)
    gather = Gather(p, tokens, cuts, ag_send.at[0], ag_recv.at[0])
    stages = range(p.nz)
    arrive = greet(plane_and_replicas(p))
    loads[0].wait()
    tokens[own] = normed_tokens(prompt_v[...].astype(jnp.float32))
    cut(0)
    with jax.named_scope("barrier"):
        arrive()

    def send(m):
        for group in (ACROSS, SAME, NEAR):
            moves[m].send(group)

    send(0)
    gather.run(0)
    for m in range(1, 3):
        cut(m)
    send(1)
    for hops in stages:
        moves[0].pass_on(hops)
    gather.run(1)
    send(2)
    for hops in stages[:2]:
        moves[1].pass_on(hops)
    for stage in stages[2:3]:
        gather.run(stage)
    for hops in stages[2:]:
        moves[1].pass_on(hops)
    for hops in stages[:2]:
        moves[2].pass_on(hops)
    for stage in stages[3:]:
        gather.run(stage)
    for m in range(3, 6):
        cut(m)
    for hops in stages[2:]:
        moves[2].pass_on(hops)
    gather.run(p.nz)
    for m in range(3, 6):
        send(m)
    for m in range(3):
        for hops in stages:
            moves[m].pass_far(hops)
    for m in range(3):
        moves[m].wait_all_here()
    outs = [pltpu.make_async_copy(first_v.at[m], served[m], out_sem.at[m]) for m in range(3)]
    for out in outs:
        out.start()

    scatter = Scatter(p, part, *scatter_refs[:3], scatter_refs[3:])
    blocks_at_once = rows_at_once // count
    tiles = p.fs // blocks_at_once
    z_at_once = blocks_at_once // p.ny

    def tile(step, carry):
        at = jnp.where(2 * p.z < p.nz, tiles - 1 - step, step)
        start = pl.multiple_of(at * rows_at_once, rows_at_once)
        ffn_rows(tokens, [first_v.at[m] for m in range(3)], part, hidden, start, scales, turned)
        scatter.send_y_of(lambda z0: z0 // z_at_once == at)
        return carry

    lax.fori_loop(0, tiles, tile, 0)
    for hops in stages:
        moves[3].pass_on(hops)
    for hops in reversed(stages):
        scatter.reduce(hops)
        if hops == min(2, p.nz - 1):
            scatter.send_own_y()
        for m in range(4, 6):
            if hops == p.nz + 3 - m:
                for d in stages:
                    moves[m].pass_on(d)
    middle = (prompt_v[...].astype(jnp.float32) + 0.5 * part[own].astype(jnp.float32)).astype(jnp.bfloat16)
    middle_out[...] = middle
    tokens_next[own] = normed_tokens(middle.astype(jnp.float32))
    gather_next = Gather(p, tokens_next, cuts, ag_send.at[1], ag_recv.at[1])

    def store(f, cut):
        piece, height = f * cuts + cut, count // cuts
        pltpu.make_async_copy(
            rows_of_block(tokens_next, piece, height), rows_of_block(tokens_out, piece, height), token_sem
        ).start()

    for stage in range(p.nz + 1):
        gather_next.run(stage, store)
    for m in range(3, 6):
        for hops in stages:
            moves[m].pass_far(hops)
    for m in range(3, 6):
        moves[m].wait_all_here()
    wait_bytes(tokens_next, token_sem)
    for out in outs:
        out.wait()
    for move in moves:
        move.drain()
    gather.drain()
    gather_next.drain()
    scatter.drain()


def first_half(prompt, gains, weights, sizes):
    gr, fs, tp = sizes
    rows, columns = weights[0].shape
    count, depth = prompt.shape
    blocks = fs // tp
    width = columns // blocks
    total = gr * fs * rows
    rows_at_once = count * fs // 2
    bf16 = jnp.bfloat16
    turned = turns(rows)
    across = (width, total) if turned else (total, width)
    piece = (width, rows) if turned else (rows, width)
    served = jax.ShapeDtypeStruct(across, bf16)
    return pl.pallas_call(
        functools.partial(first_kernel, sizes, count, rows_at_once, turned),
        out_shape=[served] * 6
        + [jax.ShapeDtypeStruct((count * fs, depth), bf16), jax.ShapeDtypeStruct((count, depth), bf16)],
        in_specs=[ANY, VMEM, VMEM] + [ANY] * 6,
        out_specs=[ANY] * 7 + [VMEM],
        scratch_shapes=[
            pltpu.VMEM((count, depth), bf16),
            pltpu.VMEM((6, rows, columns), jnp.float32),
            pltpu.VMEM((6, blocks, *piece), bf16),
            pltpu.VMEM((3, *across), bf16),
            pltpu.VMEM((count * fs, depth), bf16),
            pltpu.VMEM((count * fs, depth), bf16),
            pltpu.VMEM((count * fs, depth), bf16),
            pltpu.VMEM((rows_at_once, width), bf16),
            pltpu.SemaphoreType.DMA((7,)),
            pltpu.SemaphoreType.DMA((3,)),
            pltpu.SemaphoreType.DMA,
            pltpu.SemaphoreType.DMA((2, fs, cuts_of(count), 4)),
            pltpu.SemaphoreType.DMA((2, fs, cuts_of(count))),
            *relayout_sems(6, blocks, sizes),
            *scatter_scratch(sizes, count, depth),
        ],
        compiler_params=pltpu.CompilerParams(
            collective_id=0, has_side_effects=True, vmem_limit_bytes=VMEM_LIMIT
        ),
        name="first_half",
    )(prompt, *(gain.reshape(1, -1) for gain in gains), *weights)


def second_kernel(fs, rows_at_once, turned, *refs):
    (tokens, *served), refs = refs[:7], refs[7:]
    (*outs, part), refs = refs[:7], refs[7:]
    tokens_v, served_v, part_v, hidden, in_sem, out_sem, part_sem = refs
    width = hidden.shape[1]
    scales = scales_of(tokens.shape[1], width, fs)
    loads = {m: pltpu.make_async_copy(served[m], served_v.at[m], in_sem.at[m]) for m in (0, 1, 2, 5)}
    stores = [pltpu.make_async_copy(served_v.at[m], outs[m], out_sem.at[m]) for m in range(6)]

    def load_slab(m, i, low, high):
        slab = (pl.ds(low, high - low),) if turned else (slice(None), pl.ds(low, high - low))
        return pltpu.make_async_copy(served[m].at[slab], served_v.at[(m, *slab)], in_sem.at[7 + 2 * i + m - 3])

    slabs = slabs_of(width) if turned else [(0, width)]
    load_tokens = pltpu.make_async_copy(tokens, tokens_v, in_sem.at[6])
    load_tokens.start()
    for i, (low, high) in enumerate(slabs):
        for m in (3, 4):
            load_slab(m, i, low, high).start()
    for m in (5, 0, 1, 2):
        loads[m].start()
    load_tokens.wait()
    tiles = tokens.shape[0] // rows_at_once

    def tile(step, carry):
        def ready(i):
            @pl.when(step == 0)
            def _():
                if i is None:
                    loads[5].wait()
                elif i < len(slabs):
                    for m in (3, 4):
                        load_slab(m, i, *slabs[i]).wait()

        start = pl.multiple_of(step * rows_at_once, rows_at_once)
        weights = [served_v.at[m] for m in (3, 4, 5)]
        ffn_rows(tokens_v, weights, part_v, hidden, start, scales, turned, ready)
        rows = pl.ds(start, rows_at_once)
        pltpu.make_async_copy(part_v.at[rows], part.at[rows], part_sem).start()

        @pl.when(step == 0)
        def _():
            for m in range(3):
                loads[m].wait()
            for store in stores:
                store.start()

        return carry

    lax.fori_loop(0, tiles, tile, 0)
    wait_bytes(part_v, part_sem)
    for store in stores:
        store.wait()


def second_half(tokens, served, fs, turned):
    across = served[0].shape
    width = across[0 if turned else 1]
    count, depth = tokens.shape
    rows_at_once = count // 2
    bf16 = jnp.bfloat16
    return pl.pallas_call(
        functools.partial(second_kernel, fs, rows_at_once, turned),
        out_shape=[jax.ShapeDtypeStruct(across, bf16)] * 6
        + [jax.ShapeDtypeStruct((count, depth), bf16)],
        in_specs=[ANY] * 7,
        out_specs=[ANY] * 7,
        scratch_shapes=[
            pltpu.VMEM((count, depth), bf16),
            pltpu.VMEM((6, *across), bf16),
            pltpu.VMEM((count, depth), bf16),
            pltpu.VMEM((rows_at_once, width), bf16),
            pltpu.SemaphoreType.DMA((7 + 2 * len(slabs_of(width)),)),
            pltpu.SemaphoreType.DMA((6,)),
            pltpu.SemaphoreType.DMA,
        ],
        compiler_params=pltpu.CompilerParams(vmem_limit_bytes=VMEM_LIMIT),
        name="second_half",
    )(tokens, *served)


def last_kernel(sizes, count, partial, middle, result, part, part_sem, *scatter_refs):
    p = Place(sizes)
    scatter = Scatter(p, part, *scatter_refs[:3], scatter_refs[3:])

    def load(z0):
        rows = pl.ds(pl.multiple_of(z0 * p.ny * count, p.ny * count), p.ny * count)
        return pltpu.make_async_copy(partial.at[rows], part.at[rows], part_sem.at[z0])

    def begin(z0, sign):
        load(z0).wait()
        scatter.send_y(z0)

    arrive = greet(neighbours(p))
    for hops in range(p.nz - 1, -1, -1):
        scatter.at_distance(hops, lambda z0, sign: load(z0).start())
    arrive()
    for hops in range(p.nz - 1, 0, -1):
        scatter.at_distance(hops, begin)
    load(p.z).wait()
    for hops in range(p.nz - 1, -1, -1):
        scatter.reduce(hops)
        if hops == min(2, p.nz - 1):
            scatter.send_own_y()
    own = pl.ds(pl.multiple_of(p.f * count, count), count)
    result[...] = (
        middle[...].astype(jnp.float32) + 0.5 * part[own].astype(jnp.float32)
    ).astype(jnp.bfloat16)
    scatter.drain()


def last_step(partial, middle, sizes):
    fs = sizes[1]
    count, depth = middle.shape
    return pl.pallas_call(
        functools.partial(last_kernel, sizes, count),
        out_shape=jax.ShapeDtypeStruct((count, depth), jnp.bfloat16),
        in_specs=[ANY, VMEM],
        out_specs=VMEM,
        scratch_shapes=[
            pltpu.VMEM((fs * count, depth), jnp.bfloat16),
            pltpu.SemaphoreType.DMA((fs // inner_of(fs),)),
            *scatter_scratch(sizes, count, depth),
        ],
        compiler_params=pltpu.CompilerParams(
            collective_id=1, has_side_effects=True, vmem_limit_bytes=VMEM_LIMIT
        ),
        name="last_step",
    )(partial, middle)


def on_device(
    prompt,
    norm_first,
    gate_first,
    up_first,
    down_first,
    norm_second,
    gate_second,
    up_second,
    down_second,
):
    sizes = tuple(lax.axis_size(axis) for axis in ("gr", "fs", "tp"))
    weights = (gate_first, up_first, down_first, gate_second, up_second, down_second)
    *served, tokens, middle = first_half(prompt, (norm_first, norm_second), weights, sizes)
    turned = turns(gate_first.shape[0])
    *served, partial = second_half(tokens, served, sizes[1], turned)
    result = last_step(partial, middle, sizes)
    if turned:
        served = [block.T for block in served]
    return (*served, result)


def solution(mesh):
    in_specs = (
        P(("gr", "fs", "tp"), None),
        P(("gr", "fs")),
        P(("gr", "fs"), "tp"),
        P(("gr", "fs"), "tp"),
        P(("gr", "fs"), "tp"),
        P(("gr", "fs")),
        P(("gr", "fs"), "tp"),
        P(("gr", "fs"), "tp"),
        P(("gr", "fs"), "tp"),
    )
    out_specs = (
        P(None, "fs"),
        P(None, "fs"),
        P(None, "fs"),
        P(None, "fs"),
        P(None, "fs"),
        P(None, "fs"),
        P(("gr", "fs", "tp"), None),
    )
    return jax.shard_map(
        on_device, mesh=mesh, in_specs=in_specs, out_specs=out_specs, check_vma=False
    )
```

```python
import functools

import jax
import jax.numpy as jnp
from jax import lax
from jax.experimental import pallas as pl
from jax.experimental.pallas import tpu as pltpu
from jax.sharding import PartitionSpec as P

EPS = 1e-06
MESH = pl.DeviceIdType.MESH
VMEM_LIMIT = 63 * 1024 * 1024
CUTS = 3
SAME, NEAR, ACROSS = range(3)
ANY = pl.BlockSpec(memory_space=pl.ANY)
VMEM = pl.BlockSpec(memory_space=pltpu.VMEM)


def inner_of(fs):
    return max(n for n in range(1, fs + 1) if fs % n == 0 and n * n <= fs)


class Place:
    def __init__(self, sizes):
        self.gr, self.fs, self.tp = sizes
        self.ny = inner_of(self.fs)
        self.nz = self.fs // self.ny
        self.g, self.f, self.t = (lax.axis_index(axis) for axis in ("gr", "fs", "tp"))
        self.z = self.f // self.ny
        self.y = self.f % self.ny

    def at(self, z, y):
        return (self.g, z * self.ny + y, self.t)

    def same_half(self, z0):
        return (2 * z0 < self.nz) == (2 * self.z < self.nz)

    def partner(self, z):
        return z + 1 - 2 * (z % 2)

    def by_z(self, z, z0, cut, ends=True):
        paired = z0 == self.partner(z)
        return paired if ends and cut == 0 else paired & (z > 0) & (z < self.nz - 1)


def remote(src, dst, send_sem, recv_sem, device):
    return pltpu.make_async_remote_copy(
        src_ref=src,
        dst_ref=dst,
        send_sem=send_sem,
        recv_sem=recv_sem,
        device_id=device,
        device_id_type=MESH,
    )


def wait_bytes(ref, sem):
    pltpu.make_async_copy(ref, ref, sem).wait()


def rows_of_block(ref, f, count):
    return ref.at[pl.ds(pl.multiple_of(f * count, count), count)]


def greet(devices):
    barrier = pltpu.get_barrier_semaphore()
    expected = 0
    for valid, device in devices:

        def signal():
            pl.semaphore_signal(barrier, inc=1, device_id=device, device_id_type=MESH)

        if valid is True:
            signal()
            expected = expected + 1
        else:
            pl.when(valid)(signal)
            expected = expected + jnp.where(valid, 1, 0)
    return lambda: pl.semaphore_wait(barrier, expected)


def plane_and_replicas(p):
    for away in range(p.fs):
        for hop in range(p.tp):
            if away or hop:
                yield True, (p.g, (p.f + away) % p.fs, (p.t + hop) % p.tp)
    for hop in range(1, p.gr):
        yield True, ((p.g + hop) % p.gr, p.f, p.t)


class Relayout:
    def __init__(self, place, turned, pieces, out, sems):
        self.p, self.turned, self.pieces, self.out = place, turned, pieces, out
        self.first_send, self.first_recv, self.gr_send, self.gr_recv, self.tp_send, self.tp_recv = sems
        self.blocks, height, across = pieces.shape
        self.sub = height // place.tp
        self.rows = across if turned else height

    def rows_of(self, from_gr, from_fs, core):
        source = from_gr * self.p.fs + from_fs
        if self.turned:
            start = pl.multiple_of(source * self.rows, self.rows)
            return self.out.at[pl.ds(core * self.sub, self.sub), pl.ds(start, self.rows)]
        start = pl.multiple_of(source * self.rows + core * self.sub, self.sub)
        return self.out.at[pl.ds(start, self.sub)]

    def _first(self, step, act_local, act_far, group):
        p = self.p
        slot = (step + p.f) % self.blocks
        block = p.t * self.blocks + slot
        z0 = block // p.ny
        across = jnp.logical_not(p.same_half(z0))
        if group == SAME:
            wanted = z0 == p.z
        elif group == ACROSS:
            wanted = across
        elif group == NEAR:
            wanted = jnp.logical_not(across) & (z0 != p.z)
        for core in range(p.tp):
            mine = jnp.logical_and(block == p.f, p.t == core)
            source = self.pieces.at[slot, pl.ds(core * self.sub, self.sub)]
            target = self.rows_of(p.g, p.f, core)
            far = remote(
                source,
                target,
                self.first_send.at[slot, core],
                self.first_recv.at[p.f],
                (p.g, block, core),
            )
            if act_local is not None and group == SAME:

                @pl.when(mine)
                def _():
                    act_local(source, target)

            others = jnp.logical_not(mine)

            @pl.when(others if group is None else others & wanted)
            def _():
                act_far(far)

    @jax.named_scope("w_send")
    def send(self, group):
        def local(source, target):
            pltpu.make_async_copy(source, target, self.first_recv.at[self.p.f]).start()

        def body(step, carry):
            self._first(step, local, lambda copy: copy.start(), group)
            return carry

        lax.fori_loop(0, self.blocks, body, 0)

    def _to_peers(self, ref):
        p = self.p
        for hop in range(1, p.tp):
            remote(ref, ref, self.tp_send, self.tp_recv, (p.g, p.f, (p.t + hop) % p.tp)).start()

    def _sources(self, groups, visit):
        p = self.p

        def body(i, carry):
            source = (p.f + 2 * p.fs - i // p.tp - (i % p.tp) * self.blocks) % p.fs
            z0 = source // p.ny
            same, half = z0 == p.z, p.same_half(z0)
            kinds = {SAME: same, NEAR: half & jnp.logical_not(same), ACROSS: jnp.logical_not(half)}
            wanted = functools.reduce(jnp.logical_or, [kinds[group] for group in groups])
            pl.when(wanted)(functools.partial(visit, source))
            return carry

        lax.fori_loop(0, p.fs, body, 0)

    def pass_on(self, *groups):
        p = self.p

        def visit(source):
            ref = self.rows_of(p.g, source, p.t)
            wait_bytes(ref, self.first_recv.at[source])
            for hop in range(1, p.gr):
                remote(
                    ref,
                    ref,
                    self.gr_send,
                    self.gr_recv.at[hop - 1, source],
                    ((p.g + hop) % p.gr, p.f, p.t),
                ).start()
            self._to_peers(ref)

        with jax.named_scope(f"w_pass_on#{groups}"):
            self._sources(groups, visit)

    def pass_far(self, *groups):
        p = self.p

        def visit(source):
            for hop in range(1, p.gr):
                ref = self.rows_of((p.g + p.gr - hop) % p.gr, source, p.t)
                wait_bytes(ref, self.gr_recv.at[hop - 1, source])
                self._to_peers(ref)

        with jax.named_scope(f"w_pass_far#{groups}"):
            self._sources(groups, visit)

    def _wait_pieces(self, count, sem):
        if not count:
            return
        if self.turned:
            half = pl.ds(0, self.sub)
            per_row = self.p.gr * self.p.fs
            if count % per_row:
                wait_bytes(self.out.at[half, pl.ds(0, count * self.rows)], sem)
            else:
                wait_bytes(self.out.at[pl.ds(0, self.sub * (count // per_row))], sem)
        else:
            wait_bytes(self.out.at[pl.ds(0, count * self.sub)], sem)

    @jax.named_scope("w_wait")
    def wait_all_here(self):
        p = self.p
        self._wait_pieces(p.gr * p.fs * (p.tp - 1), self.tp_recv)

    def drain(self):
        p = self.p

        def body(step, carry):
            self._first(step, None, lambda copy: copy.wait_send(), None)
            return carry

        lax.fori_loop(0, self.blocks, body, 0)
        self._wait_pieces(p.fs * (p.gr - 1), self.gr_send)
        self._wait_pieces(p.gr * p.fs * (p.tp - 1), self.tp_send)


def relayout_sems(mats, blocks, sizes):
    gr, fs, tp = sizes
    return [
        pltpu.SemaphoreType.DMA((mats, blocks, tp)),
        pltpu.SemaphoreType.DMA((mats, fs)),
        pltpu.SemaphoreType.DMA((mats,)),
        pltpu.SemaphoreType.DMA((mats, max(gr - 1, 1), fs)),
        pltpu.SemaphoreType.DMA((mats,)),
        pltpu.SemaphoreType.DMA((mats,)),
    ]


class Gather:
    def __init__(self, place, tokens, cuts, ends, send_sem, recv_sem):
        self.p, self.tokens, self.cuts, self.ends = place, tokens, cuts, ends
        self.height = tokens.shape[0] // (place.fs * cuts)
        self.send_sem, self.recv_sem = send_sem, recv_sem

    def piece(self, f, cut):
        return rows_of_block(self.tokens, f * self.cuts + cut, self.height)

    def _along_z(self, f, cut, sign, act, also=None):
        p = self.p
        z = p.z + sign
        ref = self.piece(f, cut)
        valid = (z >= 0) & (z < p.nz)

        @pl.when(valid if also is None else valid & also)
        def _():
            way = jnp.where(sign > 0, 0, 1)
            act(remote(ref, ref, self.send_sem.at[f, cut, way], self.recv_sem.at[f, cut], p.at(z, p.y)))

    def _along_y(self, f, cut, sign, act, also=None):
        p = self.p
        y = p.y + sign
        ref = self.piece(f, cut)
        valid = (y >= 0) & (y < p.ny)

        @pl.when(valid if also is None else valid & also)
        def _():
            way = 2 if sign > 0 else 3
            act(remote(ref, ref, self.send_sem.at[f, cut, way], self.recv_sem.at[f, cut], p.at(p.z, y)))

    def _each(self, stage, half, arrive, act, done):
        p = self.p
        last = p.nz

        def column(z0, sign, cut):
            f = z0 * p.ny + p.y
            arrive(f, cut)
            self._along_z(f, cut, sign, act)
            by_y = jnp.logical_not(p.by_z(p.z, z0, cut, self.ends))
            for way in (1, -1):
                self._along_y(f, cut, way, act, by_y)
            done(f, cut)

        def row(z0, y0, sign, hops, same, cut):
            f = z0 * p.ny + y0
            arrive(f, cut)
            if hops + 1 < p.ny:
                self._along_y(f, cut, sign, act, jnp.logical_not(p.by_z(p.z, z0, cut, self.ends)))
            if same:
                other = p.partner(p.z)
                self._along_z(f, cut, other - p.z, act, p.by_z(other, p.z, cut, self.ends))
            done(f, cut)

        def rows(away):
            for hops in range(1, p.ny):
                for sign_z in (1, -1) if away else (1,):
                    z0 = p.z - sign_z * away
                    for sign in (1, -1):
                        y0 = p.y - sign * hops

                        @pl.when((z0 >= 0) & (z0 < p.nz) & (y0 >= 0) & (y0 < p.ny))
                        def _():
                            for cut in range(self.cuts):
                                row(z0, y0, sign, hops, away == 0, cut)

        if stage == 0:
            for cut in range(self.cuts):
                for sign in (1, -1):
                    self._along_z(p.f, cut, sign, act)
                    self._along_y(p.f, cut, sign, act)
                done(p.f, cut)
        elif stage < last:
            for sign in (1, -1):
                z0 = p.z - sign * stage

                valid = (z0 >= 0) & (z0 < p.nz)
                if half is not None:
                    valid = valid & (p.same_half(z0) if half else jnp.logical_not(p.same_half(z0)))

                @pl.when(valid)
                def _():
                    for cut in range(self.cuts):
                        column(z0, sign, cut)

            if stage == 1 and half is not False:
                rows(0)
        else:
            for away in range(1, p.nz):
                rows(away)

    def run(self, stage, done=lambda f, cut: None, half=None):
        with jax.named_scope(f"gather#s={stage}"):
            self._each(
                stage,
                half,
                lambda f, cut: wait_bytes(self.piece(f, cut), self.recv_sem.at[f, cut]),
                lambda copy: copy.start(),
                done,
            )

    def drain(self):
        for stage in range(self.p.nz + 1):
            self._each(stage, None, lambda f, cut: None, lambda copy: copy.wait_send(), lambda f, cut: None)


class Scatter:
    def __init__(self, place, part, y_land, z_land, row_land, sems):
        self.p, self.part, self.y_land, self.z_land, self.row_land = place, part, y_land, z_land, row_land
        self.y_send, self.y_recv, self.z_send, self.z_recv, self.row_recv = sems
        self.cuts, self.height = y_land.shape[1:3]
        self.towards = jnp.where(2 * place.z < place.nz, 1, -1)

    def rows(self, f, cut):
        return pl.ds(pl.multiple_of((f * self.cuts + cut) * self.height, self.height), self.height)

    def _y_copy(self, z0, y0, sign, cut):
        p = self.p
        f = z0 * p.ny + y0
        at = p.y + sign
        slot = f if sign < 0 else jnp.where(at == y0, p.fs + z0, f)
        return remote(
            self.part.at[self.rows(f, cut)],
            self.y_land.at[slot, cut],
            self.y_send.at[f, cut],
            self.y_recv.at[slot, cut],
            p.at(p.z, at),
        )

    def _z_copy(self, z0, sign, cut):
        p = self.p
        at = p.z + sign
        slot = jnp.where((sign > 0) & (at == z0), p.nz, z0)
        return remote(
            self.part.at[self.rows(z0 * p.ny + p.y, cut)],
            self.z_land.at[slot, cut],
            self.z_send.at[z0, cut],
            self.z_recv.at[slot, cut],
            p.at(at, p.y),
        )

    def _add(self, f, land, recv, slot, cut):
        wait_bytes(land.at[slot, cut], recv.at[slot, cut])
        rows = self.rows(f, cut)
        total = self.part[rows].astype(jnp.float32) + land[slot, cut].astype(jnp.float32)
        self.part[rows] = total.astype(jnp.bfloat16)

    def _row_copy(self, z0, y0, cut):
        p = self.p
        f = z0 * p.ny + y0
        return remote(
            self.part.at[self.rows(f, cut)],
            self.row_land.at[y0, cut],
            self.y_send.at[f, cut],
            self.row_recv.at[y0, cut],
            p.at(z0, p.y),
        )

    def send_y(self, z0):
        self._send_y(z0, False)

    def send_own_y(self):
        with jax.named_scope("own_row"):
            self._send_y(self.p.z, True)

    def _send_y(self, z0, own):
        p = self.p
        other = p.partner(p.z)
        for hops in range(p.ny - 1, 0, -1):
            for sign in (1, -1):
                y0, behind = p.y + sign * hops, p.y - sign
                valid = (y0 >= 0) & (y0 < p.ny)
                f = z0 * p.ny + y0
                for cut in range(self.cuts):
                    if own:

                        @pl.when(valid & (other < p.nz) & p.by_z(other, p.z, cut))
                        def _():
                            self._add(f, self.row_land, self.row_recv, y0, cut)

                    by_z = False if own else p.by_z(p.z, z0, cut)
                    by_y = valid if own else valid & jnp.logical_not(by_z)
                    if hops + 1 < p.ny:

                        @pl.when(by_y & (behind >= 0) & (behind < p.ny))
                        def _():
                            self._add(f, self.y_land, self.y_recv, f, cut)

                    @pl.when(by_y)
                    def _():
                        self._y_copy(z0, y0, sign, cut).start()

                    if not own:

                        @pl.when(valid & by_z)
                        def _():
                            self._row_copy(z0, y0, cut).start()

    def take_y(self, z0, cut):
        p = self.p
        f = z0 * p.ny + p.y
        by_y = jnp.logical_not(p.by_z(p.z, z0, cut))

        @pl.when(by_y & (p.y + 1 < p.ny))
        def _():
            self._add(f, self.y_land, self.y_recv, f, cut)

        @pl.when(by_y & (p.y > 0))
        def _():
            self._add(f, self.y_land, self.y_recv, p.fs + z0, cut)

    def at_distance(self, hops, visit, also=None):
        p = self.p
        for sign in (self.towards, -self.towards) if hops else (1,):
            z0 = p.z + sign * hops
            valid = (z0 >= 0) & (z0 < p.nz)
            if also is not None:
                valid = valid & also(z0)
            pl.when(valid)(functools.partial(visit, z0, sign))

    def send_y_of(self, also):
        for hops in range(self.p.nz - 1, 0, -1):
            self.at_distance(hops, lambda z0, sign: self.send_y(z0), also)

    def reduce(self, hops):
        p = self.p

        def step(z0, sign):
            behind = p.z - sign
            for cut in range(self.cuts):
                self.take_y(z0, cut)
                if hops + 1 < p.nz:

                    @pl.when((behind >= 0) & (behind < p.nz))
                    def _():
                        self._add(z0 * p.ny + p.y, self.z_land, self.z_recv, z0, cut)

                self._z_copy(z0, sign, cut).start()

        with jax.named_scope(f"reduce#d={hops}"):
            if hops:
                self.at_distance(hops, step)
                return
            for cut in range(self.cuts):
                self.take_y(p.z, cut)

                @pl.when(p.z + 1 < p.nz)
                def _():
                    self._add(p.f, self.z_land, self.z_recv, p.z, cut)

                @pl.when(p.z > 0)
                def _():
                    self._add(p.f, self.z_land, self.z_recv, p.nz, cut)

    def drain(self):
        p = self.p
        for cut in range(self.cuts):
            for z0 in range(p.nz):
                for hops in range(1, p.ny):
                    for sign in (1, -1):
                        y0 = p.y + sign * hops

                        @pl.when((y0 >= 0) & (y0 < p.ny))
                        def _():
                            self._y_copy(z0, y0, sign, cut).wait_send()

            for hops in range(1, p.nz):
                self.at_distance(hops, lambda z0, sign: self._z_copy(z0, sign, cut).wait_send())


def cuts_of(count):
    return CUTS if count % (16 * CUTS) == 0 else 1


def scatter_scratch(sizes, count, depth):
    fs = sizes[1]
    ny = inner_of(fs)
    nz = fs // ny
    cuts = cuts_of(count)
    piece = (cuts, count // cuts, depth)
    return [
        pltpu.VMEM((fs + nz, *piece), jnp.bfloat16),
        pltpu.VMEM((nz + 1, *piece), jnp.bfloat16),
        pltpu.VMEM((ny, *piece), jnp.bfloat16),
        pltpu.SemaphoreType.DMA((fs, cuts)),
        pltpu.SemaphoreType.DMA((fs + nz, cuts)),
        pltpu.SemaphoreType.DMA((nz, cuts)),
        pltpu.SemaphoreType.DMA((nz + 1, cuts)),
        pltpu.SemaphoreType.DMA((ny, cuts)),
    ]


def normed_tokens(resid_f):
    return (
        resid_f * lax.rsqrt(jnp.mean(resid_f * resid_f, axis=-1, keepdims=True) + EPS)
    ).astype(jnp.bfloat16)


def column_of(row):
    n = row.shape[1]
    across = lax.broadcasted_iota(jnp.int32, (n, n), 1)
    down = lax.broadcasted_iota(jnp.int32, (n, n), 0)
    return jnp.sum(jnp.where(across == down, row, 0.0), axis=1, keepdims=True)


@jax.named_scope("cut")
def cut_into(pieces, weight, gain, turned):
    blocks, height, width = pieces.shape
    if turned:
        value = weight[...].T
        if gain is not None:
            value = value * gain[...]
        for slot in range(blocks):
            pieces[slot] = value[slot * height : (slot + 1) * height].astype(jnp.bfloat16)
        return
    gain = None if gain is None else column_of(gain[...])
    for slot in range(blocks):
        value = weight[:, slot * width : (slot + 1) * width]
        if gain is not None:
            value = gain * value
        pieces[slot] = value.astype(jnp.bfloat16)


def slabs_of(width):
    return [(low, min(low + 256, width)) for low in range(0, width, 256)]


@jax.named_scope("ffn")
def ffn_rows(tokens, weights, part, hidden, start, scales, turned, ready=lambda i: None):
    gate, up, down = weights
    in_scale, out_scale = scales
    count, width = hidden.shape
    depth = tokens.shape[1]
    rows = pl.ds(start, count)
    inward = (((1,), (1 if turned else 0,)), ((), ()))
    outward = (((1,), (0 if turned else 1,)), ((), ()))
    for i, (low, high) in enumerate(slabs_of(width)):
        ready(i)

        def project(weight):
            block = weight[low:high, :] if turned else weight[:, low:high]
            return lax.dot_general(
                tokens[rows, :], block, inward, preferred_element_type=jnp.float32
            ) * in_scale

        gate_pre, up_pre = project(gate), project(up)
        act = gate_pre / (1.0 + jnp.exp(-gate_pre)) * up_pre
        hidden[:, low:high] = act.astype(jnp.bfloat16)
    ready(None)
    chunk = 256 if depth % 256 == 0 else depth

    def body(i, carry):
        low = pl.multiple_of(i * chunk, chunk)
        block = down[:, pl.ds(low, chunk)] if turned else down[pl.ds(low, chunk), :]
        value = lax.dot_general(hidden[...], block, outward, preferred_element_type=jnp.float32)
        part[rows, pl.ds(low, chunk)] = (value * out_scale).astype(jnp.bfloat16)
        return carry

    lax.fori_loop(0, depth // chunk, body, 0)


def scales_of(depth, width, fs):
    return depth ** (-0.5), (width * fs) ** (-0.5)


def turns(rows):
    return rows % 128 == 0


def main_kernel(sizes, count, rows_at_once, turned, *refs):
    (prompt, gain_first, gain_second, *weights), refs = refs[:9], refs[9:]
    (*served, result), refs = refs[:7], refs[7:]
    (prompt_v, weights_v, pieces, served_v, tokens, tokens_next, part, hidden, middle_v), refs = refs[:9], refs[9:]
    (in_sem, out_sem, ag_send, ag_recv, *refs) = refs
    relayout_refs, scatter_refs = refs[:6], refs[6:]
    p = Place(sizes)
    depth = tokens.shape[1]
    scales = scales_of(depth, hidden.shape[1], p.fs)

    loads = [pltpu.make_async_copy(prompt, prompt_v, in_sem.at[6])]
    loads += [pltpu.make_async_copy(weights[m], weights_v.at[m], in_sem.at[m]) for m in range(6)]
    with jax.named_scope("start"):
        for load in loads:
            load.start()

    moves = [
        Relayout(p, turned, pieces.at[m], served_v.at[m], [s.at[m] for s in relayout_refs])
        for m in range(6)
    ]
    gains = [gain_first, gain_first, None, gain_second, gain_second, None]

    def cut(m):
        loads[1 + m].wait()
        cut_into(pieces.at[m], weights_v.at[m], gains[m], turned)

    own = pl.ds(pl.multiple_of(p.f * count, count), count)
    cuts = cuts_of(count)
    gather = Gather(p, tokens, cuts, False, ag_send.at[0], ag_recv.at[0])
    stages = range(p.nz)
    arrive = greet(plane_and_replicas(p))
    loads[0].wait()
    tokens[own] = normed_tokens(prompt_v[...].astype(jnp.float32))
    cut(0)
    with jax.named_scope("barrier"):
        arrive()

    def send(m, *groups):
        for group in groups or (ACROSS, SAME, NEAR):
            moves[m].send(group)

    send(0)
    gather.run(0)
    for m in range(1, 3):
        cut(m)
    send(1, SAME, NEAR)
    send(2, SAME)
    moves[0].pass_on(SAME)
    gather.run(1, half=True)
    send(1, ACROSS)
    moves[0].pass_on(NEAR)
    moves[0].pass_on(ACROSS)
    moves[1].pass_on(SAME, NEAR)
    gather.run(1, half=False)
    send(2, ACROSS, NEAR)
    moves[2].pass_on(SAME)
    for m in range(3, 6):
        cut(m)
    for stage in stages[2:3]:
        gather.run(stage)
    moves[2].pass_on(NEAR)
    moves[1].pass_on(ACROSS)
    for stage in stages[3:]:
        gather.run(stage)
    moves[0].pass_far(SAME, NEAR, ACROSS)
    moves[2].pass_on(ACROSS)
    for m in range(3, 6):
        send(m)
    gather.run(p.nz)
    for m in range(1, 3):
        moves[m].pass_far(SAME, NEAR)
        moves[m].pass_far(ACROSS)
    for m in range(3):
        moves[m].wait_all_here()
    outs = [pltpu.make_async_copy(served_v.at[m], served[m], out_sem.at[m]) for m in range(6)]
    for m in range(3):
        outs[m].start()

    scatter = Scatter(p, part, *scatter_refs[:3], scatter_refs[3:])
    tiles = p.fs * count // rows_at_once
    z_at_once = p.nz // tiles

    def branch(source, first_weight):
        def tile(step, carry):
            at = jnp.where(2 * p.z < p.nz, tiles - 1 - step, step)
            start = pl.multiple_of(at * rows_at_once, rows_at_once)
            weights = [served_v.at[first_weight + m] for m in range(3)]
            ffn_rows(source, weights, part, hidden, start, scales, turned)
            scatter.send_y_of(lambda z0: z0 // z_at_once == at)
            return carry

        lax.fori_loop(0, tiles, tile, 0)

    branch(tokens, 0)
    moves[3].pass_on(SAME, NEAR)
    moves[3].pass_on(ACROSS)
    for hops in reversed(stages):
        scatter.reduce(hops)
        if hops == min(2, p.nz - 1):
            scatter.send_own_y()
        if hops == p.nz - 1:
            moves[4].pass_on(SAME, NEAR)
            moves[4].pass_on(ACROSS)
        if hops == min(2, p.nz - 1):
            moves[5].pass_on(SAME, NEAR)
            moves[5].pass_on(ACROSS)
    middle = (prompt_v[...].astype(jnp.float32) + 0.5 * part[own].astype(jnp.float32)).astype(jnp.bfloat16)
    middle_v[...] = middle
    tokens_next[own] = normed_tokens(middle.astype(jnp.float32))
    gather_next = Gather(p, tokens_next, cuts, True, ag_send.at[1], ag_recv.at[1])
    gather_next.run(0)
    for m in range(3, 5):
        moves[m].pass_far(SAME, NEAR, ACROSS)
    for stage in stages[1:]:
        gather_next.run(stage)
        if stage == 1:
            moves[5].pass_far(SAME, NEAR, ACROSS)
    gather_next.run(p.nz)
    for m in range(3, 6):
        moves[m].wait_all_here()
    for m in range(3, 6):
        outs[m].start()
    scatter.drain()
    branch(tokens_next, 3)
    for hops in reversed(stages):
        scatter.reduce(hops)
        if hops == min(2, p.nz - 1):
            scatter.send_own_y()
    result[...] = (
        middle_v[...].astype(jnp.float32) + 0.5 * part[own].astype(jnp.float32)
    ).astype(jnp.bfloat16)
    with jax.named_scope("drain"):
        for out in outs:
            out.wait()
        for move in moves:
            move.drain()
        gather.drain()
        gather_next.drain()
        scatter.drain()


def both_halves(prompt, gains, weights, sizes):
    gr, fs, tp = sizes
    rows, columns = weights[0].shape
    count, depth = prompt.shape
    blocks = fs // tp
    width = columns // blocks
    total = gr * fs * rows
    rows_at_once = count * fs // 2
    bf16 = jnp.bfloat16
    turned = turns(rows)
    across = (width, total) if turned else (total, width)
    piece = (width, rows) if turned else (rows, width)
    return pl.pallas_call(
        functools.partial(main_kernel, sizes, count, rows_at_once, turned),
        out_shape=[jax.ShapeDtypeStruct(across, bf16)] * 6 + [jax.ShapeDtypeStruct((count, depth), bf16)],
        in_specs=[ANY, VMEM, VMEM] + [ANY] * 6,
        out_specs=[ANY] * 6 + [VMEM],
        scratch_shapes=[
            pltpu.VMEM((count, depth), bf16),
            pltpu.VMEM((6, rows, columns), jnp.float32),
            pltpu.VMEM((6, blocks, *piece), bf16),
            pltpu.VMEM((6, *across), bf16),
            pltpu.VMEM((count * fs, depth), bf16),
            pltpu.VMEM((count * fs, depth), bf16),
            pltpu.VMEM((count * fs, depth), bf16),
            pltpu.VMEM((rows_at_once, width), bf16),
            pltpu.VMEM((count, depth), bf16),
            pltpu.SemaphoreType.DMA((7,)),
            pltpu.SemaphoreType.DMA((6,)),
            pltpu.SemaphoreType.DMA((2, fs, cuts_of(count), 4)),
            pltpu.SemaphoreType.DMA((2, fs, cuts_of(count))),
            *relayout_sems(6, blocks, sizes),
            *scatter_scratch(sizes, count, depth),
        ],
        compiler_params=pltpu.CompilerParams(
            collective_id=0, has_side_effects=True, vmem_limit_bytes=VMEM_LIMIT
        ),
        name="both_halves",
    )(prompt, *(gain.reshape(1, -1) for gain in gains), *weights)


def hand_over_kernel(parts, *refs):
    sources, targets, (held, in_sem, out_sem) = refs[:6], refs[6:12], refs[12:]
    height = held.shape[1] // parts
    pieces = [(m, i, pl.ds(i * height, height)) for m in range(6) for i in range(parts)]
    loads = [pltpu.make_async_copy(sources[m].at[rows], held.at[m, rows], in_sem.at[m, i]) for m, i, rows in pieces]
    stores = [pltpu.make_async_copy(held.at[m, rows], targets[m].at[rows], out_sem.at[m, i]) for m, i, rows in pieces]
    for load in loads:
        load.start()
    for load, store in zip(loads, stores):
        load.wait()
        store.start()
    for store in stores:
        store.wait()


def hand_over(served):
    across = served[0].shape
    parts = 2
    return pl.pallas_call(
        functools.partial(hand_over_kernel, parts),
        out_shape=[jax.ShapeDtypeStruct(across, jnp.bfloat16)] * 6,
        in_specs=[ANY] * 6,
        out_specs=[ANY] * 6,
        scratch_shapes=[
            pltpu.VMEM((6, *across), jnp.bfloat16),
            pltpu.SemaphoreType.DMA((6, parts)),
            pltpu.SemaphoreType.DMA((6, parts)),
        ],
        compiler_params=pltpu.CompilerParams(vmem_limit_bytes=VMEM_LIMIT),
        name="hand_over",
    )(*served)


def on_device(
    prompt,
    norm_first,
    gate_first,
    up_first,
    down_first,
    norm_second,
    gate_second,
    up_second,
    down_second,
):
    sizes = tuple(lax.axis_size(axis) for axis in ("gr", "fs", "tp"))
    weights = (gate_first, up_first, down_first, gate_second, up_second, down_second)
    *served, result = both_halves(prompt, (norm_first, norm_second), weights, sizes)
    served = hand_over(served)
    turned = turns(gate_first.shape[0])
    if turned:
        served = [block.T for block in served]
    return (*served, result)


def solution(mesh):
    in_specs = (
        P(("gr", "fs", "tp"), None),
        P(("gr", "fs")),
        P(("gr", "fs"), "tp"),
        P(("gr", "fs"), "tp"),
        P(("gr", "fs"), "tp"),
        P(("gr", "fs")),
        P(("gr", "fs"), "tp"),
        P(("gr", "fs"), "tp"),
        P(("gr", "fs"), "tp"),
    )
    out_specs = (
        P(None, "fs"),
        P(None, "fs"),
        P(None, "fs"),
        P(None, "fs"),
        P(None, "fs"),
        P(None, "fs"),
        P(("gr", "fs", "tp"), None),
    )
    return jax.shard_map(
        on_device, mesh=mesh, in_specs=in_specs, out_specs=out_specs, check_vma=False
    )
```

```python
import functools

import jax
import jax.numpy as jnp
from jax import lax
from jax.experimental import pallas as pl
from jax.experimental.pallas import tpu as pltpu
from jax.sharding import PartitionSpec as P

EPS = 1e-06
MESH = pl.DeviceIdType.MESH
MAIN_VMEM_LIMIT = 42 * 1024 * 1024
CUTS = 3
SAME, NEAR, ACROSS = range(3)
ANY = pl.BlockSpec(memory_space=pl.ANY)
VMEM = pl.BlockSpec(memory_space=pltpu.VMEM)


def inner_of(fs):
    return max(n for n in range(1, fs + 1) if fs % n == 0 and n * n <= fs)


class Place:
    def __init__(self, sizes):
        self.gr, self.fs, self.tp = sizes
        self.ny = inner_of(self.fs)
        self.nz = self.fs // self.ny
        self.g, self.f, self.t = (lax.axis_index(axis) for axis in ("gr", "fs", "tp"))
        self.z = self.f // self.ny
        self.y = self.f % self.ny

    def at(self, z, y):
        return (self.g, z * self.ny + y, self.t)

    def same_half(self, z0):
        return (2 * z0 < self.nz) == (2 * self.z < self.nz)

    def partner(self, z):
        return z + 1 - 2 * (z % 2)

    def by_z(self, z, z0, cut, ends=True):
        paired = z0 == self.partner(z)
        return paired if ends and cut == 0 else paired & (z > 0) & (z < self.nz - 1)


def remote(src, dst, send_sem, recv_sem, device):
    return pltpu.make_async_remote_copy(
        src_ref=src,
        dst_ref=dst,
        send_sem=send_sem,
        recv_sem=recv_sem,
        device_id=device,
        device_id_type=MESH,
    )


def wait_bytes(ref, sem):
    pltpu.make_async_copy(ref, ref, sem).wait()


def rows_of_block(ref, f, count):
    return ref.at[pl.ds(pl.multiple_of(f * count, count), count)]


def greet(devices):
    barrier = pltpu.get_barrier_semaphore()
    expected = 0
    for valid, device in devices:

        def signal():
            pl.semaphore_signal(barrier, inc=1, device_id=device, device_id_type=MESH)

        if valid is True:
            signal()
            expected = expected + 1
        else:
            pl.when(valid)(signal)
            expected = expected + jnp.where(valid, 1, 0)
    return lambda: pl.semaphore_wait(barrier, expected)


def plane_and_replicas(p):
    for away in range(p.fs):
        for hop in range(p.tp):
            if away or hop:
                yield True, (p.g, (p.f + away) % p.fs, (p.t + hop) % p.tp)
    for hop in range(1, p.gr):
        yield True, ((p.g + hop) % p.gr, p.f, p.t)


class Relayout:
    def __init__(self, place, turned, pieces, out, sems):
        self.p, self.turned, self.pieces, self.out = place, turned, pieces, out
        self.first_send, self.first_recv, self.gr_send, self.gr_recv, self.tp_send, self.tp_recv = sems
        self.blocks, height, across = pieces.shape
        self.sub = height // place.tp
        self.rows = across if turned else height

    def rows_of(self, from_gr, from_fs, core):
        source = from_gr * self.p.fs + from_fs
        if self.turned:
            start = pl.multiple_of(source * self.rows, self.rows)
            return self.out.at[pl.ds(core * self.sub, self.sub), pl.ds(start, self.rows)]
        start = pl.multiple_of(source * self.rows + core * self.sub, self.sub)
        return self.out.at[pl.ds(start, self.sub)]

    def _first(self, step, act_local, act_far, group):
        p = self.p
        slot = (step + p.f) % self.blocks
        block = p.t * self.blocks + slot
        z0 = block // p.ny
        across = jnp.logical_not(p.same_half(z0))
        if group == SAME:
            wanted = z0 == p.z
        elif group == ACROSS:
            wanted = across
        elif group == NEAR:
            wanted = jnp.logical_not(across) & (z0 != p.z)
        for core in range(p.tp):
            mine = jnp.logical_and(block == p.f, p.t == core)
            source = self.pieces.at[slot, pl.ds(core * self.sub, self.sub)]
            target = self.rows_of(p.g, p.f, core)
            far = remote(
                source,
                target,
                self.first_send.at[slot, core],
                self.first_recv.at[p.f],
                (p.g, block, core),
            )
            if act_local is not None and group == SAME:

                @pl.when(mine)
                def _():
                    act_local(source, target)

            others = jnp.logical_not(mine)

            @pl.when(others if group is None else others & wanted)
            def _():
                act_far(far)

    @jax.named_scope("w_send")
    def send(self, group):
        def local(source, target):
            pltpu.make_async_copy(source, target, self.first_recv.at[self.p.f]).start()

        def body(step, carry):
            self._first(step, local, lambda copy: copy.start(), group)
            return carry

        lax.fori_loop(0, self.blocks, body, 0)

    def _to_peers(self, ref):
        p = self.p
        for hop in range(1, p.tp):
            remote(ref, ref, self.tp_send, self.tp_recv, (p.g, p.f, (p.t + hop) % p.tp)).start()

    def _sources(self, groups, visit):
        p = self.p

        def body(i, carry):
            source = (p.f + 2 * p.fs - i // p.tp - (i % p.tp) * self.blocks) % p.fs
            z0 = source // p.ny
            same, half = z0 == p.z, p.same_half(z0)
            kinds = {SAME: same, NEAR: half & jnp.logical_not(same), ACROSS: jnp.logical_not(half)}
            wanted = functools.reduce(jnp.logical_or, [kinds[group] for group in groups])
            pl.when(wanted)(functools.partial(visit, source))
            return carry

        lax.fori_loop(0, p.fs, body, 0)

    def pass_on(self, *groups):
        p = self.p

        def visit(source):
            ref = self.rows_of(p.g, source, p.t)
            wait_bytes(ref, self.first_recv.at[source])
            for hop in range(1, p.gr):
                remote(
                    ref,
                    ref,
                    self.gr_send,
                    self.gr_recv.at[hop - 1, source],
                    ((p.g + hop) % p.gr, p.f, p.t),
                ).start()
            self._to_peers(ref)

        with jax.named_scope(f"w_pass_on#{groups}"):
            self._sources(groups, visit)

    def pass_far(self, *groups):
        p = self.p

        def visit(source):
            for hop in range(1, p.gr):
                ref = self.rows_of((p.g + p.gr - hop) % p.gr, source, p.t)
                wait_bytes(ref, self.gr_recv.at[hop - 1, source])
                self._to_peers(ref)

        with jax.named_scope(f"w_pass_far#{groups}"):
            self._sources(groups, visit)

    def _wait_pieces(self, count, sem):
        if not count:
            return
        if self.turned:
            half = pl.ds(0, self.sub)
            per_row = self.p.gr * self.p.fs
            if count % per_row:
                wait_bytes(self.out.at[half, pl.ds(0, count * self.rows)], sem)
            else:
                wait_bytes(self.out.at[pl.ds(0, self.sub * (count // per_row))], sem)
        else:
            wait_bytes(self.out.at[pl.ds(0, count * self.sub)], sem)

    @jax.named_scope("w_wait")
    def wait_all_here(self):
        p = self.p
        self._wait_pieces(p.gr * p.fs * (p.tp - 1), self.tp_recv)

    def drain(self):
        p = self.p

        def body(step, carry):
            self._first(step, None, lambda copy: copy.wait_send(), None)
            return carry

        lax.fori_loop(0, self.blocks, body, 0)
        self._wait_pieces(p.fs * (p.gr - 1), self.gr_send)
        self._wait_pieces(p.gr * p.fs * (p.tp - 1), self.tp_send)


def relayout_sems(mats, blocks, sizes):
    gr, fs, tp = sizes
    return [
        pltpu.SemaphoreType.DMA((mats, blocks, tp)),
        pltpu.SemaphoreType.DMA((mats, fs)),
        pltpu.SemaphoreType.DMA((mats,)),
        pltpu.SemaphoreType.DMA((mats, max(gr - 1, 1), fs)),
        pltpu.SemaphoreType.DMA((mats,)),
        pltpu.SemaphoreType.DMA((mats,)),
    ]


class Gather:
    def __init__(self, place, tokens, cuts, ends, send_sem, recv_sem):
        self.p, self.tokens, self.cuts, self.ends = place, tokens, cuts, ends
        self.height = tokens.shape[0] // (place.fs * cuts)
        self.send_sem, self.recv_sem = send_sem, recv_sem

    def piece(self, f, cut):
        return rows_of_block(self.tokens, f * self.cuts + cut, self.height)

    def _along_z(self, f, cut, sign, act, also=None):
        p = self.p
        z = p.z + sign
        ref = self.piece(f, cut)
        valid = (z >= 0) & (z < p.nz)

        @pl.when(valid if also is None else valid & also)
        def _():
            way = jnp.where(sign > 0, 0, 1)
            act(remote(ref, ref, self.send_sem.at[f, cut, way], self.recv_sem.at[f, cut], p.at(z, p.y)))

    def _along_y(self, f, cut, sign, act, also=None):
        p = self.p
        y = p.y + sign
        ref = self.piece(f, cut)
        valid = (y >= 0) & (y < p.ny)

        @pl.when(valid if also is None else valid & also)
        def _():
            way = 2 if sign > 0 else 3
            act(remote(ref, ref, self.send_sem.at[f, cut, way], self.recv_sem.at[f, cut], p.at(p.z, y)))

    def _each(self, stage, half, arrive, act, done):
        p = self.p
        last = p.nz

        def column(z0, sign, cut):
            f = z0 * p.ny + p.y
            arrive(f, cut)
            self._along_z(f, cut, sign, act)
            by_y = jnp.logical_not(p.by_z(p.z, z0, cut, self.ends))
            for way in (1, -1):
                self._along_y(f, cut, way, act, by_y)
            done(f, cut)

        def row(z0, y0, sign, hops, same, cut):
            f = z0 * p.ny + y0
            arrive(f, cut)
            if hops + 1 < p.ny:
                self._along_y(f, cut, sign, act, jnp.logical_not(p.by_z(p.z, z0, cut, self.ends)))
            if same:
                other = p.partner(p.z)
                self._along_z(f, cut, other - p.z, act, p.by_z(other, p.z, cut, self.ends))
            done(f, cut)

        def rows(away):
            for hops in range(1, p.ny):
                for sign_z in (1, -1) if away else (1,):
                    z0 = p.z - sign_z * away
                    for sign in (1, -1):
                        y0 = p.y - sign * hops

                        @pl.when((z0 >= 0) & (z0 < p.nz) & (y0 >= 0) & (y0 < p.ny))
                        def _():
                            for cut in range(self.cuts):
                                row(z0, y0, sign, hops, away == 0, cut)

        if stage == 0:
            for cut in range(self.cuts):
                for sign in (1, -1):
                    self._along_z(p.f, cut, sign, act)
                    self._along_y(p.f, cut, sign, act)
                done(p.f, cut)
        elif stage < last:
            for sign in (1, -1):
                z0 = p.z - sign * stage

                valid = (z0 >= 0) & (z0 < p.nz)
                if half is not None:
                    valid = valid & (p.same_half(z0) if half else jnp.logical_not(p.same_half(z0)))

                @pl.when(valid)
                def _():
                    for cut in range(self.cuts):
                        column(z0, sign, cut)

            if stage == 1 and half is not False:
                rows(0)
        else:
            for away in range(1, p.nz):
                rows(away)

    def run(self, stage, done=lambda f, cut: None, half=None):
        with jax.named_scope(f"gather#s={stage}"):
            self._each(
                stage,
                half,
                lambda f, cut: wait_bytes(self.piece(f, cut), self.recv_sem.at[f, cut]),
                lambda copy: copy.start(),
                done,
            )

    def drain(self):
        for stage in range(self.p.nz + 1):
            self._each(stage, None, lambda f, cut: None, lambda copy: copy.wait_send(), lambda f, cut: None)


class Scatter:
    def __init__(self, place, part, y_land, z_land, row_land, sems):
        self.p, self.part, self.y_land, self.z_land, self.row_land = place, part, y_land, z_land, row_land
        self.y_send, self.y_recv, self.z_send, self.z_recv, self.row_recv = sems
        self.cuts, self.height = y_land.shape[1:3]
        self.towards = jnp.where(2 * place.z < place.nz, 1, -1)

    def rows(self, f, cut):
        return pl.ds(pl.multiple_of((f * self.cuts + cut) * self.height, self.height), self.height)

    def _y_copy(self, z0, y0, sign, cut):
        p = self.p
        f = z0 * p.ny + y0
        at = p.y + sign
        slot = f if sign < 0 else jnp.where(at == y0, p.fs + z0, f)
        return remote(
            self.part.at[self.rows(f, cut)],
            self.y_land.at[slot, cut],
            self.y_send.at[f, cut],
            self.y_recv.at[slot, cut],
            p.at(p.z, at),
        )

    def _z_copy(self, z0, sign, cut):
        p = self.p
        at = p.z + sign
        slot = jnp.where((sign > 0) & (at == z0), p.nz, z0)
        return remote(
            self.part.at[self.rows(z0 * p.ny + p.y, cut)],
            self.z_land.at[slot, cut],
            self.z_send.at[z0, cut],
            self.z_recv.at[slot, cut],
            p.at(at, p.y),
        )

    def _add(self, f, land, recv, slot, cut):
        wait_bytes(land.at[slot, cut], recv.at[slot, cut])
        rows = self.rows(f, cut)
        total = self.part[rows].astype(jnp.float32) + land[slot, cut].astype(jnp.float32)
        self.part[rows] = total.astype(jnp.bfloat16)

    def _row_copy(self, z0, y0, cut):
        p = self.p
        f = z0 * p.ny + y0
        return remote(
            self.part.at[self.rows(f, cut)],
            self.row_land.at[y0, cut],
            self.y_send.at[f, cut],
            self.row_recv.at[y0, cut],
            p.at(z0, p.y),
        )

    def send_y(self, z0):
        self._send_y(z0, False)

    def send_own_y(self):
        with jax.named_scope("own_row"):
            self._send_y(self.p.z, True)

    def _send_y(self, z0, own):
        p = self.p
        other = p.partner(p.z)
        for hops in range(p.ny - 1, 0, -1):
            for sign in (1, -1):
                y0, behind = p.y + sign * hops, p.y - sign
                valid = (y0 >= 0) & (y0 < p.ny)
                f = z0 * p.ny + y0
                for cut in range(self.cuts):
                    if own:

                        @pl.when(valid & (other < p.nz) & p.by_z(other, p.z, cut))
                        def _():
                            self._add(f, self.row_land, self.row_recv, y0, cut)

                    by_z = False if own else p.by_z(p.z, z0, cut)
                    by_y = valid if own else valid & jnp.logical_not(by_z)
                    if hops + 1 < p.ny:

                        @pl.when(by_y & (behind >= 0) & (behind < p.ny))
                        def _():
                            self._add(f, self.y_land, self.y_recv, f, cut)

                    @pl.when(by_y)
                    def _():
                        self._y_copy(z0, y0, sign, cut).start()

                    if not own:

                        @pl.when(valid & by_z)
                        def _():
                            self._row_copy(z0, y0, cut).start()

    def take_y(self, z0, cut):
        p = self.p
        f = z0 * p.ny + p.y
        by_y = jnp.logical_not(p.by_z(p.z, z0, cut))

        @pl.when(by_y & (p.y + 1 < p.ny))
        def _():
            self._add(f, self.y_land, self.y_recv, f, cut)

        @pl.when(by_y & (p.y > 0))
        def _():
            self._add(f, self.y_land, self.y_recv, p.fs + z0, cut)

    def at_distance(self, hops, visit, also=None):
        p = self.p
        for sign in (self.towards, -self.towards) if hops else (1,):
            z0 = p.z + sign * hops
            valid = (z0 >= 0) & (z0 < p.nz)
            if also is not None:
                valid = valid & also(z0)
            pl.when(valid)(functools.partial(visit, z0, sign))

    def send_y_of(self, also):
        for hops in range(self.p.nz - 1, 0, -1):
            self.at_distance(hops, lambda z0, sign: self.send_y(z0), also)

    def reduce(self, hops):
        p = self.p

        def step(z0, sign):
            behind = p.z - sign
            for cut in range(self.cuts):
                self.take_y(z0, cut)
                if hops + 1 < p.nz:

                    @pl.when((behind >= 0) & (behind < p.nz))
                    def _():
                        self._add(z0 * p.ny + p.y, self.z_land, self.z_recv, z0, cut)

                self._z_copy(z0, sign, cut).start()

        with jax.named_scope(f"reduce#d={hops}"):
            if hops:
                self.at_distance(hops, step)
                return
            for cut in range(self.cuts):
                self.take_y(p.z, cut)

                @pl.when(p.z + 1 < p.nz)
                def _():
                    self._add(p.f, self.z_land, self.z_recv, p.z, cut)

                @pl.when(p.z > 0)
                def _():
                    self._add(p.f, self.z_land, self.z_recv, p.nz, cut)

    def drain(self):
        p = self.p
        for cut in range(self.cuts):
            for z0 in range(p.nz):
                for hops in range(1, p.ny):
                    for sign in (1, -1):
                        y0 = p.y + sign * hops

                        @pl.when((y0 >= 0) & (y0 < p.ny))
                        def _():
                            self._y_copy(z0, y0, sign, cut).wait_send()

            for hops in range(1, p.nz):
                self.at_distance(hops, lambda z0, sign: self._z_copy(z0, sign, cut).wait_send())


def cuts_of(count):
    return CUTS if count % (16 * CUTS) == 0 else 1


def scatter_scratch(sizes, count, depth):
    fs = sizes[1]
    ny = inner_of(fs)
    nz = fs // ny
    cuts = cuts_of(count)
    piece = (cuts, count // cuts, depth)
    return [
        pltpu.VMEM((fs + nz, *piece), jnp.bfloat16),
        pltpu.VMEM((nz + 1, *piece), jnp.bfloat16),
        pltpu.VMEM((ny, *piece), jnp.bfloat16),
        pltpu.SemaphoreType.DMA((fs, cuts)),
        pltpu.SemaphoreType.DMA((fs + nz, cuts)),
        pltpu.SemaphoreType.DMA((nz, cuts)),
        pltpu.SemaphoreType.DMA((nz + 1, cuts)),
        pltpu.SemaphoreType.DMA((ny, cuts)),
    ]


def normed_tokens(resid_f):
    return (
        resid_f * lax.rsqrt(jnp.mean(resid_f * resid_f, axis=-1, keepdims=True) + EPS)
    ).astype(jnp.bfloat16)


def column_of(row):
    n = row.shape[1]
    across = lax.broadcasted_iota(jnp.int32, (n, n), 1)
    down = lax.broadcasted_iota(jnp.int32, (n, n), 0)
    return jnp.sum(jnp.where(across == down, row, 0.0), axis=1, keepdims=True)


@jax.named_scope("cut")
def cut_into(pieces, weight, gain, turned):
    blocks, height, width = pieces.shape
    if turned:
        value = weight[...].T
        if gain is not None:
            value = value * gain[...]
        for slot in range(blocks):
            pieces[slot] = value[slot * height : (slot + 1) * height].astype(jnp.bfloat16)
        return
    gain = None if gain is None else column_of(gain[...])
    for slot in range(blocks):
        value = weight[:, slot * width : (slot + 1) * width]
        if gain is not None:
            value = gain * value
        pieces[slot] = value.astype(jnp.bfloat16)


def slabs_of(width):
    return [(low, min(low + 256, width)) for low in range(0, width, 256)]


@jax.named_scope("ffn")
def ffn_rows(tokens, weights, part, hidden, start, scales, turned, ready=lambda i: None):
    gate, up, down = weights
    in_scale, out_scale = scales
    count, width = hidden.shape
    depth = tokens.shape[1]
    rows = pl.ds(start, count)
    inward = (((1,), (1 if turned else 0,)), ((), ()))
    outward = (((1,), (0 if turned else 1,)), ((), ()))
    for i, (low, high) in enumerate(slabs_of(width)):
        ready(i)

        def project(weight):
            block = weight[low:high, :] if turned else weight[:, low:high]
            return lax.dot_general(
                tokens[rows, :], block, inward, preferred_element_type=jnp.float32
            ) * in_scale

        gate_pre, up_pre = project(gate), project(up)
        act = gate_pre / (1.0 + jnp.exp(-gate_pre)) * up_pre
        hidden[:, low:high] = act.astype(jnp.bfloat16)
    ready(None)
    chunk = 256 if depth % 256 == 0 else depth

    def body(i, carry):
        low = pl.multiple_of(i * chunk, chunk)
        block = down[:, pl.ds(low, chunk)] if turned else down[pl.ds(low, chunk), :]
        value = lax.dot_general(hidden[...], block, outward, preferred_element_type=jnp.float32)
        part[rows, pl.ds(low, chunk)] = (value * out_scale).astype(jnp.bfloat16)
        return carry

    lax.fori_loop(0, depth // chunk, body, 0)


def scales_of(depth, width, fs):
    return depth ** (-0.5), (width * fs) ** (-0.5)


def turns(rows):
    return rows % 128 == 0


def main_kernel(sizes, count, rows_at_once, turned, *refs):
    (prompt, gain_first, gain_second, *weights), refs = refs[:9], refs[9:]
    (*served, result), refs = refs[:7], refs[7:]
    (prompt_v, weights_v, pieces, tokens, tokens_next, part, hidden, middle_v), refs = refs[:8], refs[8:]
    (in_sem, ag_send, ag_recv, *refs) = refs
    relayout_refs, scatter_refs = refs[:6], refs[6:]
    p = Place(sizes)
    depth = tokens.shape[1]
    scales = scales_of(depth, hidden.shape[1], p.fs)

    loads = [pltpu.make_async_copy(prompt, prompt_v, in_sem.at[6])]
    loads += [pltpu.make_async_copy(weights[m], weights_v.at[m], in_sem.at[m]) for m in range(6)]
    with jax.named_scope("start"):
        for load in loads:
            load.start()

    moves = [
        Relayout(p, turned, pieces.at[m], served[m], [s.at[m] for s in relayout_refs])
        for m in range(6)
    ]
    gains = [gain_first, gain_first, None, gain_second, gain_second, None]

    def cut(m):
        loads[1 + m].wait()
        cut_into(pieces.at[m], weights_v.at[m], gains[m], turned)

    own = pl.ds(pl.multiple_of(p.f * count, count), count)
    cuts = cuts_of(count)
    gather = Gather(p, tokens, cuts, False, ag_send.at[0], ag_recv.at[0])
    stages = range(p.nz)
    arrive = greet(plane_and_replicas(p))
    loads[0].wait()
    tokens[own] = normed_tokens(prompt_v[...].astype(jnp.float32))
    cut(0)
    with jax.named_scope("barrier"):
        arrive()

    def send(m, *groups):
        for group in groups or (ACROSS, SAME, NEAR):
            moves[m].send(group)

    send(0)
    gather.run(0)
    for m in range(1, 3):
        cut(m)
    send(1, SAME, NEAR)
    send(2, SAME)
    moves[0].pass_on(SAME)
    gather.run(1, half=True)
    send(1, ACROSS)
    moves[0].pass_on(NEAR)
    moves[0].pass_on(ACROSS)
    moves[1].pass_on(SAME, NEAR)
    gather.run(1, half=False)
    send(2, ACROSS, NEAR)
    moves[2].pass_on(SAME)
    for m in range(3, 6):
        cut(m)
    for stage in stages[2:3]:
        gather.run(stage)
    moves[2].pass_on(NEAR)
    moves[1].pass_on(ACROSS)
    for stage in stages[3:]:
        gather.run(stage)
    moves[0].pass_far(SAME, NEAR, ACROSS)
    moves[2].pass_on(ACROSS)
    for m in range(3, 6):
        send(m)
    gather.run(p.nz)
    for m in range(1, 3):
        moves[m].pass_far(SAME, NEAR)
        moves[m].pass_far(ACROSS)
    for m in range(3):
        moves[m].wait_all_here()
    scatter = Scatter(p, part, *scatter_refs[:3], scatter_refs[3:])
    tiles = p.fs * count // rows_at_once
    z_at_once = p.nz // tiles

    def branch(source, first_weight):
        def tile(step, carry):
            at = jnp.where(2 * p.z < p.nz, tiles - 1 - step, step)
            start = pl.multiple_of(at * rows_at_once, rows_at_once)
            weights = served[first_weight : first_weight + 3]
            ffn_rows(source, weights, part, hidden, start, scales, turned)
            scatter.send_y_of(lambda z0: z0 // z_at_once == at)
            return carry

        lax.fori_loop(0, tiles, tile, 0)

    branch(tokens, 0)
    moves[3].pass_on(SAME, NEAR)
    moves[3].pass_on(ACROSS)
    for hops in reversed(stages):
        scatter.reduce(hops)
        if hops == min(2, p.nz - 1):
            scatter.send_own_y()
        if hops == p.nz - 1:
            moves[4].pass_on(SAME, NEAR)
            moves[4].pass_on(ACROSS)
        if hops == min(2, p.nz - 1):
            moves[5].pass_on(SAME, NEAR)
            moves[5].pass_on(ACROSS)
    middle = (prompt_v[...].astype(jnp.float32) + 0.5 * part[own].astype(jnp.float32)).astype(jnp.bfloat16)
    middle_v[...] = middle
    tokens_next[own] = normed_tokens(middle.astype(jnp.float32))
    gather_next = Gather(p, tokens_next, cuts, True, ag_send.at[1], ag_recv.at[1])
    gather_next.run(0)
    for m in range(3, 5):
        moves[m].pass_far(SAME, NEAR, ACROSS)
    for stage in stages[1:]:
        gather_next.run(stage)
        if stage == 1:
            moves[5].pass_far(SAME, NEAR, ACROSS)
    gather_next.run(p.nz)
    for m in range(3, 6):
        moves[m].wait_all_here()
    scatter.drain()
    branch(tokens_next, 3)
    for hops in reversed(stages):
        scatter.reduce(hops)
        if hops == min(2, p.nz - 1):
            scatter.send_own_y()
    result[...] = (
        middle_v[...].astype(jnp.float32) + 0.5 * part[own].astype(jnp.float32)
    ).astype(jnp.bfloat16)
    with jax.named_scope("drain"):
        for move in moves:
            move.drain()
        gather.drain()
        gather_next.drain()
        scatter.drain()


def both_halves(prompt, gains, weights, sizes):
    gr, fs, tp = sizes
    rows, columns = weights[0].shape
    count, depth = prompt.shape
    blocks = fs // tp
    width = columns // blocks
    total = gr * fs * rows
    rows_at_once = count * fs // 2
    bf16 = jnp.bfloat16
    turned = turns(rows)
    across = (width, total) if turned else (total, width)
    piece = (width, rows) if turned else (rows, width)
    return pl.pallas_call(
        functools.partial(main_kernel, sizes, count, rows_at_once, turned),
        out_shape=[pltpu.VMEM(across, bf16)] * 6 + [pltpu.VMEM((count, depth), bf16)],
        in_specs=[ANY, VMEM, VMEM] + [ANY] * 6,
        out_specs=[VMEM] * 7,
        scratch_shapes=[
            pltpu.VMEM((count, depth), bf16),
            pltpu.VMEM((6, rows, columns), jnp.float32),
            pltpu.VMEM((6, blocks, *piece), bf16),
            pltpu.VMEM((count * fs, depth), bf16),
            pltpu.VMEM((count * fs, depth), bf16),
            pltpu.VMEM((count * fs, depth), bf16),
            pltpu.VMEM((rows_at_once, width), bf16),
            pltpu.VMEM((count, depth), bf16),
            pltpu.SemaphoreType.DMA((7,)),
            pltpu.SemaphoreType.DMA((2, fs, cuts_of(count), 4)),
            pltpu.SemaphoreType.DMA((2, fs, cuts_of(count))),
            *relayout_sems(6, blocks, sizes),
            *scatter_scratch(sizes, count, depth),
        ],
        compiler_params=pltpu.CompilerParams(
            collective_id=0, has_side_effects=True, vmem_limit_bytes=MAIN_VMEM_LIMIT
        ),
        name="both_halves",
    )(prompt, *(gain.reshape(1, -1) for gain in gains), *weights)


def hand_over_kernel(*refs):
    count = len(refs) // 2
    sources, targets, sem = refs[:count], refs[count : 2 * count], refs[2 * count]
    stores = [pltpu.make_async_copy(sources[m], targets[m], sem.at[m]) for m in range(count)]
    for store in stores:
        store.start()
    for store in stores:
        store.wait()


def hand_over(results):
    return pl.pallas_call(
        hand_over_kernel,
        out_shape=[jax.ShapeDtypeStruct(block.shape, block.dtype) for block in results],
        in_specs=[VMEM] * len(results),
        out_specs=[ANY] * len(results),
        scratch_shapes=[pltpu.SemaphoreType.DMA((len(results),))],
        compiler_params=pltpu.CompilerParams(vmem_limit_bytes=4 * 1024 * 1024),
        name="hand_over",
    )(*results)


def on_device(
    prompt,
    norm_first,
    gate_first,
    up_first,
    down_first,
    norm_second,
    gate_second,
    up_second,
    down_second,
):
    sizes = tuple(lax.axis_size(axis) for axis in ("gr", "fs", "tp"))
    weights = (gate_first, up_first, down_first, gate_second, up_second, down_second)
    results = both_halves(prompt, (norm_first, norm_second), weights, sizes)
    *served, result = hand_over(results)
    turned = turns(gate_first.shape[0])
    if turned:
        served = [block.T for block in served]
    return (*served, result)


def solution(mesh):
    in_specs = (
        P(("gr", "fs", "tp"), None),
        P(("gr", "fs")),
        P(("gr", "fs"), "tp"),
        P(("gr", "fs"), "tp"),
        P(("gr", "fs"), "tp"),
        P(("gr", "fs")),
        P(("gr", "fs"), "tp"),
        P(("gr", "fs"), "tp"),
        P(("gr", "fs"), "tp"),
    )
    out_specs = (
        P(None, "fs"),
        P(None, "fs"),
        P(None, "fs"),
        P(None, "fs"),
        P(None, "fs"),
        P(None, "fs"),
        P(("gr", "fs", "tp"), None),
    )
    return jax.shard_map(
        on_device, mesh=mesh, in_specs=in_specs, out_specs=out_specs, check_vma=False
    )
```

```python
import functools

import jax
import jax.numpy as jnp
from jax import lax
from jax.experimental import pallas as pl
from jax.experimental.pallas import tpu as pltpu
from jax.sharding import PartitionSpec as P

EPS = 1e-06
MESH = pl.DeviceIdType.MESH
MAIN_VMEM_LIMIT = 42 * 1024 * 1024
CUTS = 3
SAME, NEAR, ACROSS = range(3)
ANY = pl.BlockSpec(memory_space=pl.ANY)
VMEM = pl.BlockSpec(memory_space=pltpu.VMEM)


def inner_of(fs):
    return max(n for n in range(1, fs + 1) if fs % n == 0 and n * n <= fs)


class Place:
    def __init__(self, sizes):
        self.gr, self.fs, self.tp = sizes
        self.ny = inner_of(self.fs)
        self.nz = self.fs // self.ny
        self.g, self.f, self.t = (lax.axis_index(axis) for axis in ("gr", "fs", "tp"))
        self.z = self.f // self.ny
        self.y = self.f % self.ny

    def at(self, z, y):
        return (self.g, z * self.ny + y, self.t)

    def same_half(self, z0):
        return (2 * z0 < self.nz) == (2 * self.z < self.nz)

    def partner(self, z):
        return z + 1 - 2 * (z % 2)

    def by_z(self, z, z0, cut, ends=True):
        paired = z0 == self.partner(z)
        return paired if ends and cut == 0 else paired & (z > 0) & (z < self.nz - 1)


def remote(src, dst, send_sem, recv_sem, device):
    return pltpu.make_async_remote_copy(
        src_ref=src,
        dst_ref=dst,
        send_sem=send_sem,
        recv_sem=recv_sem,
        device_id=device,
        device_id_type=MESH,
    )


def wait_bytes(ref, sem):
    pltpu.make_async_copy(ref, ref, sem).wait()


def rows_of_block(ref, f, count):
    return ref.at[pl.ds(pl.multiple_of(f * count, count), count)]


def greet(devices):
    barrier = pltpu.get_barrier_semaphore()
    expected = 0
    for valid, device in devices:

        def signal():
            pl.semaphore_signal(barrier, inc=1, device_id=device, device_id_type=MESH)

        if valid is True:
            signal()
            expected = expected + 1
        else:
            pl.when(valid)(signal)
            expected = expected + jnp.where(valid, 1, 0)
    return lambda: pl.semaphore_wait(barrier, expected)


def plane_and_replicas(p):
    for away in range(p.fs):
        for hop in range(p.tp):
            if away or hop:
                yield True, (p.g, (p.f + away) % p.fs, (p.t + hop) % p.tp)
    for hop in range(1, p.gr):
        yield True, ((p.g + hop) % p.gr, p.f, p.t)


class Relayout:
    def __init__(self, place, turned, pieces, out, sems):
        self.p, self.turned, self.pieces, self.out = place, turned, pieces, out
        self.first_send, self.first_recv, self.gr_send, self.gr_recv, self.tp_send, self.tp_recv = sems
        self.blocks, height, across = pieces.shape
        self.sub = height // place.tp
        self.rows = across if turned else height

    def rows_of(self, from_gr, from_fs, core):
        source = from_gr * self.p.fs + from_fs
        if self.turned:
            start = pl.multiple_of(source * self.rows, self.rows)
            return self.out.at[pl.ds(core * self.sub, self.sub), pl.ds(start, self.rows)]
        start = pl.multiple_of(source * self.rows + core * self.sub, self.sub)
        return self.out.at[pl.ds(start, self.sub)]

    def _first(self, step, act_local, act_far, group):
        p = self.p
        slot = (step + p.f) % self.blocks
        block = p.t * self.blocks + slot
        z0 = block // p.ny
        across = jnp.logical_not(p.same_half(z0))
        if group == SAME:
            wanted = z0 == p.z
        elif group == ACROSS:
            wanted = across
        elif group == NEAR:
            wanted = jnp.logical_not(across) & (z0 != p.z)
        for core in range(p.tp):
            mine = jnp.logical_and(block == p.f, p.t == core)
            source = self.pieces.at[slot, pl.ds(core * self.sub, self.sub)]
            target = self.rows_of(p.g, p.f, core)
            far = remote(
                source,
                target,
                self.first_send.at[slot, core],
                self.first_recv.at[p.f],
                (p.g, block, core),
            )
            if act_local is not None and group == SAME:

                @pl.when(mine)
                def _():
                    act_local(source, target)

            others = jnp.logical_not(mine)

            @pl.when(others if group is None else others & wanted)
            def _():
                act_far(far)

    @jax.named_scope("w_send")
    def send(self, group):
        def local(source, target):
            pltpu.make_async_copy(source, target, self.first_recv.at[self.p.f]).start()

        def body(step, carry):
            self._first(step, local, lambda copy: copy.start(), group)
            return carry

        lax.fori_loop(0, self.blocks, body, 0)

    def _to_peers(self, ref):
        p = self.p
        for hop in range(1, p.tp):
            remote(ref, ref, self.tp_send, self.tp_recv, (p.g, p.f, (p.t + hop) % p.tp)).start()

    def _sources(self, groups, visit):
        p = self.p

        def body(i, carry):
            source = (p.f + 2 * p.fs - i // p.tp - (i % p.tp) * self.blocks) % p.fs
            z0 = source // p.ny
            same, half = z0 == p.z, p.same_half(z0)
            kinds = {SAME: same, NEAR: half & jnp.logical_not(same), ACROSS: jnp.logical_not(half)}
            wanted = functools.reduce(jnp.logical_or, [kinds[group] for group in groups])
            pl.when(wanted)(functools.partial(visit, source))
            return carry

        lax.fori_loop(0, p.fs, body, 0)

    def pass_on(self, *groups):
        p = self.p

        def visit(source):
            ref = self.rows_of(p.g, source, p.t)
            wait_bytes(ref, self.first_recv.at[source])
            for hop in range(1, p.gr):
                remote(
                    ref,
                    ref,
                    self.gr_send,
                    self.gr_recv.at[hop - 1, source],
                    ((p.g + hop) % p.gr, p.f, p.t),
                ).start()
            self._to_peers(ref)

        with jax.named_scope(f"w_pass_on#{groups}"):
            self._sources(groups, visit)

    def pass_far(self, *groups):
        p = self.p

        def visit(source):
            for hop in range(1, p.gr):
                ref = self.rows_of((p.g + p.gr - hop) % p.gr, source, p.t)
                wait_bytes(ref, self.gr_recv.at[hop - 1, source])
                self._to_peers(ref)

        with jax.named_scope(f"w_pass_far#{groups}"):
            self._sources(groups, visit)

    def _wait_pieces(self, count, sem):
        if not count:
            return
        if self.turned:
            half = pl.ds(0, self.sub)
            per_row = self.p.gr * self.p.fs
            if count % per_row:
                wait_bytes(self.out.at[half, pl.ds(0, count * self.rows)], sem)
            else:
                wait_bytes(self.out.at[pl.ds(0, self.sub * (count // per_row))], sem)
        else:
            wait_bytes(self.out.at[pl.ds(0, count * self.sub)], sem)

    @jax.named_scope("w_wait")
    def wait_all_here(self):
        p = self.p
        self._wait_pieces(p.gr * p.fs * (p.tp - 1), self.tp_recv)

    def drain(self):
        p = self.p

        def body(step, carry):
            self._first(step, None, lambda copy: copy.wait_send(), None)
            return carry

        lax.fori_loop(0, self.blocks, body, 0)
        self._wait_pieces(p.fs * (p.gr - 1), self.gr_send)
        self._wait_pieces(p.gr * p.fs * (p.tp - 1), self.tp_send)


def relayout_sems(mats, blocks, sizes):
    gr, fs, tp = sizes
    return [
        pltpu.SemaphoreType.DMA((mats, blocks, tp)),
        pltpu.SemaphoreType.DMA((mats, fs)),
        pltpu.SemaphoreType.DMA((mats,)),
        pltpu.SemaphoreType.DMA((mats, max(gr - 1, 1), fs)),
        pltpu.SemaphoreType.DMA((mats,)),
        pltpu.SemaphoreType.DMA((mats,)),
    ]


class Gather:
    def __init__(self, place, tokens, cuts, ends, send_sem, recv_sem):
        self.p, self.tokens, self.cuts, self.ends = place, tokens, cuts, ends
        self.height = tokens.shape[0] // (place.fs * cuts)
        self.send_sem, self.recv_sem = send_sem, recv_sem

    def piece(self, f, cut):
        return rows_of_block(self.tokens, f * self.cuts + cut, self.height)

    def _along_z(self, f, cut, sign, act, also=None):
        p = self.p
        z = p.z + sign
        ref = self.piece(f, cut)
        valid = (z >= 0) & (z < p.nz)

        @pl.when(valid if also is None else valid & also)
        def _():
            way = jnp.where(sign > 0, 0, 1)
            act(remote(ref, ref, self.send_sem.at[f, cut, way], self.recv_sem.at[f, cut], p.at(z, p.y)))

    def _along_y(self, f, cut, sign, act, also=None):
        p = self.p
        y = p.y + sign
        ref = self.piece(f, cut)
        valid = (y >= 0) & (y < p.ny)

        @pl.when(valid if also is None else valid & also)
        def _():
            way = 2 if sign > 0 else 3
            act(remote(ref, ref, self.send_sem.at[f, cut, way], self.recv_sem.at[f, cut], p.at(p.z, y)))

    def _each(self, stage, half, arrive, act, done):
        p = self.p
        last = p.nz

        def column(z0, sign, cut):
            f = z0 * p.ny + p.y
            arrive(f, cut)
            self._along_z(f, cut, sign, act)
            by_y = jnp.logical_not(p.by_z(p.z, z0, cut, self.ends))
            for way in (1, -1):
                self._along_y(f, cut, way, act, by_y)
            done(f, cut)

        def row(z0, y0, sign, hops, same, cut):
            f = z0 * p.ny + y0
            arrive(f, cut)
            if hops + 1 < p.ny:
                self._along_y(f, cut, sign, act, jnp.logical_not(p.by_z(p.z, z0, cut, self.ends)))
            if same:
                other = p.partner(p.z)
                self._along_z(f, cut, other - p.z, act, p.by_z(other, p.z, cut, self.ends))
            done(f, cut)

        def rows(away):
            for hops in range(1, p.ny):
                for sign_z in (1, -1) if away else (1,):
                    z0 = p.z - sign_z * away
                    for sign in (1, -1):
                        y0 = p.y - sign * hops

                        @pl.when((z0 >= 0) & (z0 < p.nz) & (y0 >= 0) & (y0 < p.ny))
                        def _():
                            for cut in range(self.cuts):
                                row(z0, y0, sign, hops, away == 0, cut)

        if stage == 0:
            for cut in range(self.cuts):
                for sign in (1, -1):
                    self._along_z(p.f, cut, sign, act)
                    self._along_y(p.f, cut, sign, act)
                done(p.f, cut)
        elif stage < last:
            for sign in (1, -1):
                z0 = p.z - sign * stage

                valid = (z0 >= 0) & (z0 < p.nz)
                if half is not None:
                    valid = valid & (p.same_half(z0) if half else jnp.logical_not(p.same_half(z0)))

                @pl.when(valid)
                def _():
                    for cut in range(self.cuts):
                        column(z0, sign, cut)

            if stage == 1 and half is not False:
                rows(0)
        else:
            for away in range(1, p.nz):
                rows(away)

    def run(self, stage, done=lambda f, cut: None, half=None):
        with jax.named_scope(f"gather#s={stage}"):
            self._each(
                stage,
                half,
                lambda f, cut: wait_bytes(self.piece(f, cut), self.recv_sem.at[f, cut]),
                lambda copy: copy.start(),
                done,
            )

    def drain(self):
        for stage in range(self.p.nz + 1):
            self._each(stage, None, lambda f, cut: None, lambda copy: copy.wait_send(), lambda f, cut: None)


class Scatter:
    def __init__(self, place, part, y_land, z_land, row_land, sems):
        self.p, self.part, self.y_land, self.z_land, self.row_land = place, part, y_land, z_land, row_land
        self.y_send, self.y_recv, self.z_send, self.z_recv, self.row_recv = sems
        self.cuts, self.height = y_land.shape[1:3]
        self.towards = jnp.where(2 * place.z < place.nz, 1, -1)

    def rows(self, f, cut):
        return pl.ds(pl.multiple_of((f * self.cuts + cut) * self.height, self.height), self.height)

    def _y_copy(self, z0, y0, sign, cut):
        p = self.p
        f = z0 * p.ny + y0
        at = p.y + sign
        slot = f if sign < 0 else jnp.where(at == y0, p.fs + z0, f)
        return remote(
            self.part.at[self.rows(f, cut)],
            self.y_land.at[slot, cut],
            self.y_send.at[f, cut],
            self.y_recv.at[slot, cut],
            p.at(p.z, at),
        )

    def _z_copy(self, z0, sign, cut):
        p = self.p
        at = p.z + sign
        slot = jnp.where((sign > 0) & (at == z0), p.nz, z0)
        return remote(
            self.part.at[self.rows(z0 * p.ny + p.y, cut)],
            self.z_land.at[slot, cut],
            self.z_send.at[z0, cut],
            self.z_recv.at[slot, cut],
            p.at(at, p.y),
        )

    def _add(self, f, land, recv, slot, cut):
        wait_bytes(land.at[slot, cut], recv.at[slot, cut])
        rows = self.rows(f, cut)
        total = self.part[rows].astype(jnp.float32) + land[slot, cut].astype(jnp.float32)
        self.part[rows] = total.astype(jnp.bfloat16)

    def _row_copy(self, z0, y0, cut):
        p = self.p
        f = z0 * p.ny + y0
        return remote(
            self.part.at[self.rows(f, cut)],
            self.row_land.at[y0, cut],
            self.y_send.at[f, cut],
            self.row_recv.at[y0, cut],
            p.at(z0, p.y),
        )

    def send_y(self, z0):
        self._send_y(z0, False)

    def send_own_y(self):
        with jax.named_scope("own_row"):
            self._send_y(self.p.z, True)

    def _send_y(self, z0, own):
        p = self.p
        other = p.partner(p.z)
        for hops in range(p.ny - 1, 0, -1):
            for sign in (1, -1):
                y0, behind = p.y + sign * hops, p.y - sign
                valid = (y0 >= 0) & (y0 < p.ny)
                f = z0 * p.ny + y0
                for cut in range(self.cuts):
                    if own:

                        @pl.when(valid & (other < p.nz) & p.by_z(other, p.z, cut))
                        def _():
                            self._add(f, self.row_land, self.row_recv, y0, cut)

                    by_z = False if own else p.by_z(p.z, z0, cut)
                    by_y = valid if own else valid & jnp.logical_not(by_z)
                    if hops + 1 < p.ny:

                        @pl.when(by_y & (behind >= 0) & (behind < p.ny))
                        def _():
                            self._add(f, self.y_land, self.y_recv, f, cut)

                    @pl.when(by_y)
                    def _():
                        self._y_copy(z0, y0, sign, cut).start()

                    if not own:

                        @pl.when(valid & by_z)
                        def _():
                            self._row_copy(z0, y0, cut).start()

    def take_y(self, z0, cut):
        p = self.p
        f = z0 * p.ny + p.y
        by_y = jnp.logical_not(p.by_z(p.z, z0, cut))

        @pl.when(by_y & (p.y + 1 < p.ny))
        def _():
            self._add(f, self.y_land, self.y_recv, f, cut)

        @pl.when(by_y & (p.y > 0))
        def _():
            self._add(f, self.y_land, self.y_recv, p.fs + z0, cut)

    def at_distance(self, hops, visit, also=None):
        p = self.p
        for sign in (self.towards, -self.towards) if hops else (1,):
            z0 = p.z + sign * hops
            valid = (z0 >= 0) & (z0 < p.nz)
            if also is not None:
                valid = valid & also(z0)
            pl.when(valid)(functools.partial(visit, z0, sign))

    def send_y_of(self, also):
        for hops in range(self.p.nz - 1, 0, -1):
            self.at_distance(hops, lambda z0, sign: self.send_y(z0), also)

    def reduce(self, hops):
        p = self.p

        def step(z0, sign):
            behind = p.z - sign
            for cut in range(self.cuts):
                self.take_y(z0, cut)
                if hops + 1 < p.nz:

                    @pl.when((behind >= 0) & (behind < p.nz))
                    def _():
                        self._add(z0 * p.ny + p.y, self.z_land, self.z_recv, z0, cut)

                self._z_copy(z0, sign, cut).start()

        with jax.named_scope(f"reduce#d={hops}"):
            if hops:
                self.at_distance(hops, step)
                return
            for cut in range(self.cuts):
                self.take_y(p.z, cut)

                @pl.when(p.z + 1 < p.nz)
                def _():
                    self._add(p.f, self.z_land, self.z_recv, p.z, cut)

                @pl.when(p.z > 0)
                def _():
                    self._add(p.f, self.z_land, self.z_recv, p.nz, cut)

    def drain(self):
        p = self.p
        for cut in range(self.cuts):
            for z0 in range(p.nz):
                for hops in range(1, p.ny):
                    for sign in (1, -1):
                        y0 = p.y + sign * hops

                        @pl.when((y0 >= 0) & (y0 < p.ny))
                        def _():
                            self._y_copy(z0, y0, sign, cut).wait_send()

            for hops in range(1, p.nz):
                self.at_distance(hops, lambda z0, sign: self._z_copy(z0, sign, cut).wait_send())


def cuts_of(count):
    return CUTS if count % (16 * CUTS) == 0 else 1


def scatter_scratch(sizes, count, depth):
    fs = sizes[1]
    ny = inner_of(fs)
    nz = fs // ny
    cuts = cuts_of(count)
    piece = (cuts, count // cuts, depth)
    return [
        pltpu.VMEM((fs + nz, *piece), jnp.bfloat16),
        pltpu.VMEM((nz + 1, *piece), jnp.bfloat16),
        pltpu.VMEM((ny, *piece), jnp.bfloat16),
        pltpu.SemaphoreType.DMA((fs, cuts)),
        pltpu.SemaphoreType.DMA((fs + nz, cuts)),
        pltpu.SemaphoreType.DMA((nz, cuts)),
        pltpu.SemaphoreType.DMA((nz + 1, cuts)),
        pltpu.SemaphoreType.DMA((ny, cuts)),
    ]


def normed_tokens(resid_f):
    return (
        resid_f * lax.rsqrt(jnp.mean(resid_f * resid_f, axis=-1, keepdims=True) + EPS)
    ).astype(jnp.bfloat16)


def column_of(row):
    n = row.shape[1]
    across = lax.broadcasted_iota(jnp.int32, (n, n), 1)
    down = lax.broadcasted_iota(jnp.int32, (n, n), 0)
    return jnp.sum(jnp.where(across == down, row, 0.0), axis=1, keepdims=True)


@jax.named_scope("cut")
def cut_into(pieces, weight, gain, turned):
    blocks, height, width = pieces.shape
    if turned:
        value = weight[...].T
        if gain is not None:
            value = value * gain[...]
        for slot in range(blocks):
            pieces[slot] = value[slot * height : (slot + 1) * height].astype(jnp.bfloat16)
        return
    gain = None if gain is None else column_of(gain[...])
    for slot in range(blocks):
        value = weight[:, slot * width : (slot + 1) * width]
        if gain is not None:
            value = gain * value
        pieces[slot] = value.astype(jnp.bfloat16)


def slabs_of(width):
    return [(low, min(low + 256, width)) for low in range(0, width, 256)]


@jax.named_scope("ffn")
def ffn_rows(tokens, weights, part, hidden, start, scales, turned, ready=lambda i: None):
    gate, up, down = weights
    in_scale, out_scale = scales
    count, width = hidden.shape
    depth = tokens.shape[1]
    rows = pl.ds(start, count)
    inward = (((1,), (1 if turned else 0,)), ((), ()))
    outward = (((1,), (0 if turned else 1,)), ((), ()))
    for i, (low, high) in enumerate(slabs_of(width)):
        ready(i)

        def project(weight):
            block = weight[low:high, :] if turned else weight[:, low:high]
            return lax.dot_general(
                tokens[rows, :], block, inward, preferred_element_type=jnp.float32
            ) * in_scale

        gate_pre, up_pre = project(gate), project(up)
        act = gate_pre / (1.0 + jnp.exp(-gate_pre)) * up_pre
        hidden[:, low:high] = act.astype(jnp.bfloat16)
    ready(None)
    chunk = 512 if depth % 512 == 0 else depth

    def body(i, carry):
        low = pl.multiple_of(i * chunk, chunk)
        block = down[:, pl.ds(low, chunk)] if turned else down[pl.ds(low, chunk), :]
        value = lax.dot_general(hidden[...], block, outward, preferred_element_type=jnp.float32)
        part[rows, pl.ds(low, chunk)] = (value * out_scale).astype(jnp.bfloat16)
        return carry

    lax.fori_loop(0, depth // chunk, body, 0)


def scales_of(depth, width, fs):
    return depth ** (-0.5), (width * fs) ** (-0.5)


def turns(rows):
    return rows % 128 == 0


def main_kernel(sizes, count, rows_at_once, turned, *refs):
    (prompt, gain_first, gain_second, *weights), refs = refs[:9], refs[9:]
    (*served, result), refs = refs[:7], refs[7:]
    (prompt_v, weights_v, pieces, tokens, tokens_next, part, hidden, middle_v), refs = refs[:8], refs[8:]
    (in_sem, ag_send, ag_recv, *refs) = refs
    relayout_refs, scatter_refs = refs[:6], refs[6:]
    p = Place(sizes)
    depth = tokens.shape[1]
    scales = scales_of(depth, hidden.shape[1], p.fs)

    loads = [pltpu.make_async_copy(prompt, prompt_v, in_sem.at[6])]
    loads += [pltpu.make_async_copy(weights[m], weights_v.at[m], in_sem.at[m]) for m in range(6)]
    with jax.named_scope("start"):
        for load in loads:
            load.start()

    moves = [
        Relayout(p, turned, pieces.at[m], served[m], [s.at[m] for s in relayout_refs])
        for m in range(6)
    ]
    gains = [gain_first, gain_first, None, gain_second, gain_second, None]

    def cut(m):
        loads[1 + m].wait()
        cut_into(pieces.at[m], weights_v.at[m], gains[m], turned)

    own = pl.ds(pl.multiple_of(p.f * count, count), count)
    cuts = cuts_of(count)
    gather = Gather(p, tokens, cuts, False, ag_send.at[0], ag_recv.at[0])
    stages = range(p.nz)
    arrive = greet(plane_and_replicas(p))
    loads[0].wait()
    tokens[own] = normed_tokens(prompt_v[...].astype(jnp.float32))
    cut(0)
    with jax.named_scope("barrier"):
        arrive()

    def send(m, *groups):
        for group in groups or (ACROSS, SAME, NEAR):
            moves[m].send(group)

    send(0)
    gather.run(0)
    for m in range(1, 3):
        cut(m)
    send(1, SAME, NEAR)
    send(2, SAME)
    moves[0].pass_on(SAME)
    gather.run(1, half=True)
    send(1, ACROSS)
    moves[0].pass_on(NEAR)
    moves[0].pass_on(ACROSS)
    moves[1].pass_on(SAME, NEAR)
    gather.run(1, half=False)
    send(2, ACROSS, NEAR)
    moves[2].pass_on(SAME)
    for m in range(3, 6):
        cut(m)
    for stage in stages[2:3]:
        gather.run(stage)
    moves[2].pass_on(NEAR)
    moves[1].pass_on(ACROSS)
    for stage in stages[3:]:
        gather.run(stage)
    moves[0].pass_far(SAME, NEAR, ACROSS)
    moves[2].pass_on(ACROSS)
    for m in range(3, 6):
        send(m)
    gather.run(p.nz)
    for m in range(1, 3):
        moves[m].pass_far(SAME, NEAR)
        moves[m].pass_far(ACROSS)
    for m in range(3):
        moves[m].wait_all_here()
    scatter = Scatter(p, part, *scatter_refs[:3], scatter_refs[3:])
    tiles = p.fs * count // rows_at_once
    z_at_once = p.nz // tiles

    def branch(source, first_weight):
        def tile(step, carry):
            at = jnp.where(2 * p.z < p.nz, tiles - 1 - step, step)
            start = pl.multiple_of(at * rows_at_once, rows_at_once)
            weights = served[first_weight : first_weight + 3]
            ffn_rows(source, weights, part, hidden, start, scales, turned)
            scatter.send_y_of(lambda z0: z0 // z_at_once == at)
            return carry

        lax.fori_loop(0, tiles, tile, 0)

    branch(tokens, 0)
    moves[3].pass_on(SAME, NEAR)
    moves[3].pass_on(ACROSS)
    for hops in reversed(stages):
        scatter.reduce(hops)
        if hops == min(2, p.nz - 1):
            scatter.send_own_y()
        if hops == p.nz - 1:
            moves[4].pass_on(SAME, NEAR)
            moves[4].pass_on(ACROSS)
        if hops == min(2, p.nz - 1):
            moves[5].pass_on(SAME, NEAR)
            moves[5].pass_on(ACROSS)
    middle = (prompt_v[...].astype(jnp.float32) + 0.5 * part[own].astype(jnp.float32)).astype(jnp.bfloat16)
    middle_v[...] = middle
    tokens_next[own] = normed_tokens(middle.astype(jnp.float32))
    gather_next = Gather(p, tokens_next, cuts, True, ag_send.at[1], ag_recv.at[1])
    gather_next.run(0)
    for m in range(3, 5):
        moves[m].pass_far(SAME, NEAR, ACROSS)
    for stage in stages[1:]:
        gather_next.run(stage)
        if stage == 1:
            moves[5].pass_far(SAME, NEAR, ACROSS)
    gather_next.run(p.nz)
    for m in range(3, 6):
        moves[m].wait_all_here()
    scatter.drain()
    branch(tokens_next, 3)
    for hops in reversed(stages):
        scatter.reduce(hops)
        if hops == min(2, p.nz - 1):
            scatter.send_own_y()
    result[...] = (
        middle_v[...].astype(jnp.float32) + 0.5 * part[own].astype(jnp.float32)
    ).astype(jnp.bfloat16)
    with jax.named_scope("drain"):
        for move in moves:
            move.drain()
        gather.drain()
        gather_next.drain()
        scatter.drain()


def both_halves(prompt, gains, weights, sizes):
    gr, fs, tp = sizes
    rows, columns = weights[0].shape
    count, depth = prompt.shape
    blocks = fs // tp
    width = columns // blocks
    total = gr * fs * rows
    rows_at_once = count * fs // 2
    bf16 = jnp.bfloat16
    turned = turns(rows)
    across = (width, total) if turned else (total, width)
    piece = (width, rows) if turned else (rows, width)
    return pl.pallas_call(
        functools.partial(main_kernel, sizes, count, rows_at_once, turned),
        out_shape=[pltpu.VMEM(across, bf16)] * 6 + [pltpu.VMEM((count, depth), bf16)],
        in_specs=[ANY, VMEM, VMEM] + [ANY] * 6,
        out_specs=[VMEM] * 7,
        scratch_shapes=[
            pltpu.VMEM((count, depth), bf16),
            pltpu.VMEM((6, rows, columns), jnp.float32),
            pltpu.VMEM((6, blocks, *piece), bf16),
            pltpu.VMEM((count * fs, depth), bf16),
            pltpu.VMEM((count * fs, depth), bf16),
            pltpu.VMEM((count * fs, depth), bf16),
            pltpu.VMEM((rows_at_once, width), bf16),
            pltpu.VMEM((count, depth), bf16),
            pltpu.SemaphoreType.DMA((7,)),
            pltpu.SemaphoreType.DMA((2, fs, cuts_of(count), 4)),
            pltpu.SemaphoreType.DMA((2, fs, cuts_of(count))),
            *relayout_sems(6, blocks, sizes),
            *scatter_scratch(sizes, count, depth),
        ],
        compiler_params=pltpu.CompilerParams(
            collective_id=0, has_side_effects=True, vmem_limit_bytes=MAIN_VMEM_LIMIT
        ),
        name="both_halves",
    )(prompt, *(gain.reshape(1, -1) for gain in gains), *weights)


def hand_over_kernel(*refs):
    count = len(refs) // 2
    sources, targets, sem = refs[:count], refs[count : 2 * count], refs[2 * count]
    stores = [pltpu.make_async_copy(sources[m], targets[m], sem.at[m]) for m in range(count)]
    for store in stores:
        store.start()
    for store in stores:
        store.wait()


def hand_over(results):
    return pl.pallas_call(
        hand_over_kernel,
        out_shape=[jax.ShapeDtypeStruct(block.shape, block.dtype) for block in results],
        in_specs=[VMEM] * len(results),
        out_specs=[ANY] * len(results),
        scratch_shapes=[pltpu.SemaphoreType.DMA((len(results),))],
        compiler_params=pltpu.CompilerParams(vmem_limit_bytes=4 * 1024 * 1024),
        name="hand_over",
    )(*results)


def on_device(
    prompt,
    norm_first,
    gate_first,
    up_first,
    down_first,
    norm_second,
    gate_second,
    up_second,
    down_second,
):
    sizes = tuple(lax.axis_size(axis) for axis in ("gr", "fs", "tp"))
    weights = (gate_first, up_first, down_first, gate_second, up_second, down_second)
    results = both_halves(prompt, (norm_first, norm_second), weights, sizes)
    *served, result = hand_over(results)
    turned = turns(gate_first.shape[0])
    if turned:
        served = [block.T for block in served]
    return (*served, result)


def solution(mesh):
    in_specs = (
        P(("gr", "fs", "tp"), None),
        P(("gr", "fs")),
        P(("gr", "fs"), "tp"),
        P(("gr", "fs"), "tp"),
        P(("gr", "fs"), "tp"),
        P(("gr", "fs")),
        P(("gr", "fs"), "tp"),
        P(("gr", "fs"), "tp"),
        P(("gr", "fs"), "tp"),
    )
    out_specs = (
        P(None, "fs"),
        P(None, "fs"),
        P(None, "fs"),
        P(None, "fs"),
        P(None, "fs"),
        P(None, "fs"),
        P(("gr", "fs", "tp"), None),
    )
    return jax.shard_map(
        on_device, mesh=mesh, in_specs=in_specs, out_specs=out_specs, check_vma=False
    )
```
